256 devices in a mesh: ep: 128 (over z, y, x), tp: 2 (over core).
Axes of the slice: x: 4, y: 4, z: 8, core: 2. Of those that a mesh axis runs over, the one named last changes fastest.
Arguments:
- residual_in: bfloat16 [2048, 1024], P('ep'), may hold values from -6 to 6
- lengths: int32 [2048], P('ep'), may hold values from 64 to 1024
- cache_keys: bfloat16 [2048, 2, 1024, 128], P('ep', 'tp'), may hold values from -7 to 7
- cache_values: bfloat16 [2048, 2, 1024, 128], P('ep', 'tp'), may hold values from -6 to 6
- attend_gain: bfloat16 [1024], replicated, may hold values from 0.099609375 to 1.8984375
- query_proj: bfloat16 [1024, 512], P(None, 'tp'), may hold values from -0.1875 to 0.1875
- key_proj: bfloat16 [1024, 256], P(None, 'tp'), may hold values from -0.1875 to 0.1875
- value_proj: bfloat16 [1024, 256], P(None, 'tp'), may hold values from -0.1875 to 0.1875
- lambdas: float32 [4], P('tp'), may hold values from 0.3 to 0.8
- head_gain: bfloat16 [128], replicated, may hold values from 0.099609375 to 1.8984375
- out_proj: bfloat16 [512, 1024], P('tp'), may hold values from -0.25 to 0.25
- channel_gain: bfloat16 [1024], replicated, may hold values from 0.099609375 to 1.8984375
- routes: int32 [2048, 6], P('ep'), may hold values from 0 to 127, all different within a row; in each aligned block of 16 rows (0 to 15, 16 to 31, ...) at most 2 rows name the same one
- route_weight: float32 [2048, 6], P('ep'), may hold values from 0.1 to 1
- expert_gate: bfloat16 [128, 1024, 512], P('ep', None, 'tp'), may hold values from -0.1875 to 0.1875
- expert_up: bfloat16 [128, 1024, 512], P('ep', None, 'tp'), may hold values from -0.1875 to 0.1875
- expert_down: bfloat16 [128, 512, 1024], P('ep', 'tp'), may hold values from -0.25 to 0.25
- dense_gate: bfloat16 [1024, 4096], P(None, ('ep', 'tp')), may hold values from -0.1875 to 0.1875
- dense_up: bfloat16 [1024, 4096], P(None, ('ep', 'tp')), may hold values from -0.1875 to 0.1875
- dense_down: bfloat16 [4096, 1024], P(('ep', 'tp')), may hold values from -0.09375 to 0.09375
- dense_mixer: bfloat16 [1024], replicated, may hold values from -0.1875 to 0.1875
Outputs:
- residual_out: bfloat16 [2048, 1024], P('ep')
- new_keys: bfloat16 [2048, 2, 128], P('ep', 'tp')
- new_values: bfloat16 [2048, 2, 128], P('ep', 'tp')
The draws below stay inside these ranges and needn't reach their ends.
Inputs may be any that keep to these rules, and one draw needn't show every extreme that they name: `routes`: each row names 6 different experts; in each aligned block of 16 rows (the rows of one index of ep) no expert is named by more than 2 rows, and in some blocks one expert is named by exactly 2 rows.
All inputs are finite; a program needn't handle non-finite values.
Results may differ from the reference program's by a relative error of at most 0.015.
Values may be sent and summed in bfloat16 or wider, within the bound.
A program may use at most 64 MiB of HBM per device.

```python
import math
import jax
import jax.numpy as jnp
import numpy as np
from jax import lax

D = 1024
HEADS = 4
KV_HEADS = 2
HEAD = 64
VALUE = 128
EXPERT_FF = 512
DENSE_FF = 4096
TOPK = 6
SEQ_DEV = 16
LEN = 1024
TOKENS = 2048
EXPERTS = 128
CAP = 2
N_EP = 128
N_TP = 2


def set_ends(values, own_key, low, high):
    index_at = [jax.random.randint(jax.random.fold_in(own_key, axis), (), 0, length) for axis, length in enumerate(values.shape)]
    longest = values.shape.index(max(values.shape))
    next_to = index_at[:longest] + [(index_at[longest] + 1) % values.shape[longest]] + index_at[longest + 1:]
    return values.at[tuple(index_at)].set(low).at[tuple(next_to)].set(high)


def block_levels(stream_key, shape, shards, smallest, largest):
    level = 1.0
    for dim, parts in shards:
        heights = jax.random.uniform(jax.random.fold_in(jax.random.fold_in(stream_key, 6), dim), (parts,), jnp.float32, smallest / len(shards), largest / len(shards))
        level = level * jnp.repeat(jnp.exp(heights), shape[dim] // parts).reshape((-1,) + (1,) * (len(shape) - 1 - dim))
    return level


def shared_out(stream_key, own, number, rows, amount, top, bound, skew):
    order = jax.random.permutation(stream_key, amount)
    heavy_load, common = load_shares(amount, rows * top, bound, skew, True), load_shares(amount, rows * top, bound, skew, False)
    places = jnp.arange(amount)

    def named(sizes, rotation):
        used = int((sizes > 0).sum())
        fixed = max(1, used // 4)
        shifted = fixed + (places - fixed + rotation * (used - fixed)) % max(1, amount - fixed)
        return jnp.zeros((amount,), jnp.int32).at[order[jnp.where(places < fixed, places, shifted)]].set(jnp.asarray(sizes, jnp.int32))

    sizes = jnp.where(number % 4 == 0, named(heavy_load, number // 4), named(common, number - number // 4 - 1))
    mixed = jax.random.permutation(jax.random.fold_in(own, 3), amount)
    donor, taker = mixed[0:amount // 2 * 2:2], mixed[1:amount // 2 * 2:2]
    room = jnp.minimum(sizes[donor] - 1, bound - sizes[taker]) // 2
    room = jnp.where((donor == order[0]) | (taker == order[0]) | (sizes[taker] == 0), 0, jnp.maximum(room, 0))
    shifted = jax.random.randint(jax.random.fold_in(own, 4), (amount // 2,), 0, 1 << 20) % (room + 1)
    sizes = sizes.at[donor].add(-shifted).at[taker].add(shifted)
    items = jnp.searchsorted(jnp.cumsum(sizes), jnp.arange(rows * top), side="right").astype(jnp.int32)
    listing = items.reshape(top, rows).T
    listing = listing[jax.random.permutation(jax.random.fold_in(own, 1), rows)]
    rotation = jax.random.randint(jax.random.fold_in(own, 2), (rows, 1), 0, top)
    return jnp.take_along_axis(listing, (jnp.arange(top)[None, :] + rotation) % top, axis=1)


def load_shares(count, total, limit, skew, full):
    loads = [(1 << 20) // math.isqrt(standing ** skew) + 1 for standing in range(1, count + 1)]
    largest = limit if full else min(limit, max(-(-total // count), total * loads[0] // sum(loads)))
    least = 1 if total - largest >= count - 1 else 0
    given, spare = [largest] + [least] * (count - 1), total - largest - least * (count - 1)
    while spare > 0:
        candidates = [i for i in range(1, count) if given[i] < largest] or [i for i in range(1, count) if given[i] < limit]
        whole, remaining = sum([loads[i] for i in candidates]), spare
        for i in candidates:
            more = min(limit - given[i], max(1, remaining * loads[i] // whole), spare)
            given[i] = given[i] + more
            spare = spare - more
    return np.array(given)


def normal_values(stream_key, shape, spread, bound, pieces=(), kind=jnp.bfloat16):
    values = spread * jax.random.normal(stream_key, shape, jnp.float32)
    if pieces:
        values = values * block_levels(stream_key, shape, pieces, -0.22, 0.18)
    return jnp.clip(values, -bound, bound).astype(kind)


def setup_inputs(seed: int = 0) -> dict:
    key_list = jax.random.split(jax.random.key(seed), 22)
    residual_in = normal_values(key_list[0], (TOKENS, D), 1.0, 6.0, ((0, 128),))
    lengths = set_ends(jax.random.randint(key_list[1], (TOKENS,), LEN // 16, LEN + 1), jax.random.fold_in(key_list[1], 1), LEN // 16, LEN).astype(jnp.int32)
    cache_keys = normal_values(key_list[2], (TOKENS, KV_HEADS, LEN, 2 * HEAD), 1.75, 7.0, ((0, 128), (1, 2)))
    cache_values = normal_values(key_list[3], (TOKENS, KV_HEADS, LEN, VALUE), 1.0, 6.0, ((0, 128), (1, 2)))
    attend_gain = jnp.clip(1.0 + 0.18 * jax.random.normal(key_list[4], (D,), jnp.float32), 0.099609375, 1.8984375).astype(jnp.bfloat16)
    query_proj = normal_values(key_list[5], (D, HEADS * 2 * HEAD), D ** -0.5, 0.1875, ((1, 2),))
    key_proj = normal_values(key_list[6], (D, KV_HEADS * 2 * HEAD), D ** -0.5, 0.1875, ((1, 2),))
    value_proj = normal_values(key_list[7], (D, KV_HEADS * VALUE), D ** -0.5, 0.1875, ((1, 2),))
    lambdas = jnp.clip(0.3 + 0.5 * jax.random.uniform(key_list[8], (HEADS,), jnp.float32) ** block_levels(key_list[8], (HEADS,), ((0, 2),), -0.2, 0.2), 0.3, 0.8)
    head_gain = jnp.clip(1.0 + 0.18 * jax.random.normal(key_list[9], (VALUE,), jnp.float32), 0.099609375, 1.8984375).astype(jnp.bfloat16)
    out_proj = normal_values(key_list[10], (HEADS * VALUE, D), (HEADS * VALUE) ** -0.5, 0.25, ((0, 2),))
    channel_gain = jnp.clip(1.0 + 0.18 * jax.random.normal(key_list[11], (D,), jnp.float32), 0.099609375, 1.8984375).astype(jnp.bfloat16)
    routes_keys = jax.random.split(jax.random.fold_in(key_list[12], 1), TOKENS // SEQ_DEV)
    routes_turns = jax.random.permutation(jax.random.fold_in(key_list[12], 3), TOKENS // SEQ_DEV)
    routes = jax.vmap(lambda own, number: shared_out(jax.random.fold_in(key_list[12], 2), own, number, SEQ_DEV, EXPERTS, TOPK, CAP, 2))(routes_keys, routes_turns).reshape((TOKENS, TOPK))
    route_weight = jnp.clip(jnp.exp(math.log(1.0) - 2.3025851 * jax.random.uniform(key_list[13], (TOKENS, TOPK), jnp.float32) ** block_levels(key_list[13], (TOKENS, TOPK), ((0, 128),), -0.2, 0.2)), 0.1, 1.0)
    expert_gate = normal_values(key_list[14], (EXPERTS, D, EXPERT_FF), D ** -0.5, 0.1875, ((0, 128), (2, 2)))
    expert_up = normal_values(key_list[15], (EXPERTS, D, EXPERT_FF), D ** -0.5, 0.1875, ((0, 128), (2, 2)))
    expert_down = normal_values(key_list[16], (EXPERTS, EXPERT_FF, D), EXPERT_FF ** -0.5, 0.25, ((0, 128), (1, 2)))
    dense_gate = normal_values(key_list[17], (D, DENSE_FF), D ** -0.5, 0.1875, ((1, 256),))
    dense_up = normal_values(key_list[18], (D, DENSE_FF), D ** -0.5, 0.1875, ((1, 256),))
    dense_down = normal_values(key_list[19], (DENSE_FF, D), DENSE_FF ** -0.5, 0.09375, ((0, 256),))
    dense_mixer = normal_values(key_list[20], (D,), D ** -0.5, 0.1875)
    return {"residual_in": residual_in, "lengths": lengths, "cache_keys": cache_keys, "cache_values": cache_values, "attend_gain": attend_gain, "query_proj": query_proj, "key_proj": key_proj, "value_proj": value_proj, "lambdas": lambdas, "head_gain": head_gain, "out_proj": out_proj, "channel_gain": channel_gain, "routes": routes, "route_weight": route_weight, "expert_gate": expert_gate, "expert_up": expert_up, "expert_down": expert_down, "dense_gate": dense_gate, "dense_up": dense_up, "dense_down": dense_down, "dense_mixer": dense_mixer}


NORM_EPSILON = 1e-06
ROTARY_BASE = 10000.0
HEAD_SCALE = 0.8

def norm_scale(vectors, gain_vector):
    mean_square = lax.optimization_barrier(jnp.mean(vectors * vectors, axis=-1, keepdims=True))
    return vectors * lax.rsqrt(mean_square + NORM_EPSILON) * gain_vector

def rotate(vectors, position):
    half_width = vectors.shape[-1] // 2
    inverse = ROTARY_BASE ** (-jnp.arange(half_width, dtype=jnp.float32) / half_width)
    angles = position[..., None] * inverse
    cosine = jnp.cos(angles)
    sine_part = jnp.sin(angles)
    front_half = vectors[..., :half_width]
    back_half = vectors[..., half_width:]
    return jnp.concatenate([front_half * cosine - back_half * sine_part, back_half * cosine + front_half * sine_part], axis=-1)

def rounded(values):
    return lax.optimization_barrier(values.astype(jnp.bfloat16)).astype(jnp.float32)

def reference(residual_in, lengths, cache_keys, cache_values, attend_gain, query_proj, key_proj, value_proj, lambdas, head_gain, out_proj, channel_gain, routes, route_weight, expert_gate, expert_up, expert_down, dense_gate, dense_up, dense_down, dense_mixer):
    residual = residual_in.astype(jnp.float32)
    normed = norm_scale(residual, attend_gain.astype(jnp.float32)).astype(jnp.bfloat16)
    queries = jnp.dot(normed, query_proj, preferred_element_type=jnp.float32).reshape(TOKENS, HEADS, 2, HEAD)
    key_rows = jnp.dot(normed, key_proj, preferred_element_type=jnp.float32).reshape(TOKENS, KV_HEADS, 2, HEAD)
    new_values = jnp.dot(normed, value_proj, preferred_element_type=jnp.float32).astype(jnp.bfloat16).reshape(TOKENS, KV_HEADS, VALUE)
    position = lengths.astype(jnp.float32)[:, None, None]
    queries = rotate(queries, position).astype(jnp.bfloat16)
    new_keys = rotate(key_rows, position).astype(jnp.bfloat16)
    group_size = HEADS // KV_HEADS
    mixing = lambdas.astype(jnp.float32).reshape(KV_HEADS, group_size)[None, :, :, None]
    score_scale = HEAD ** (-0.5)

    def attend(block):
        block_queries, block_keys, block_values, cached_keys, cached_values, block_lengths = block
        grouped = block_queries.astype(jnp.float32).reshape(SEQ_DEV, KV_HEADS, group_size, 2, HEAD)
        cached = cached_keys.astype(jnp.float32).reshape(SEQ_DEV, KV_HEADS, LEN, 2, HEAD)
        scores = jnp.einsum('sagmd,salmd->sagml', grouped, cached) * score_scale
        own_score = jnp.einsum('sagmd,samd->sagm', grouped, block_keys.astype(jnp.float32)) * score_scale
        visible = (jnp.arange(LEN).astype(jnp.int32)[None, :] < block_lengths.astype(jnp.int32)[:, None])[:, None, None, None, :]
        exponent = jnp.where(visible, jnp.exp(scores), 0.0)
        own_exponent = jnp.exp(own_score)
        denominator = lax.optimization_barrier(jnp.sum(exponent, axis=-1)) + own_exponent
        probability = exponent / denominator[..., None]
        own_probability = own_exponent / denominator
        weight = (probability[..., 0, :] - mixing * probability[..., 1, :]).astype(jnp.bfloat16)
        own_weight = (own_probability[..., 0] - mixing[..., 0] * own_probability[..., 1]).astype(jnp.bfloat16)
        attended = jnp.einsum('sagl,sale->sage', weight.astype(jnp.float32), cached_values.astype(jnp.float32))
        return attended + own_weight.astype(jnp.float32)[..., None] * block_values.astype(jnp.float32)[:, :, None, :]
    blocks = (queries.reshape(N_EP, SEQ_DEV, HEADS, 2, HEAD), new_keys.reshape(N_EP, SEQ_DEV, KV_HEADS, 2, HEAD), new_values.reshape(N_EP, SEQ_DEV, KV_HEADS, VALUE), cache_keys.reshape(N_EP, SEQ_DEV, KV_HEADS, LEN, 2 * HEAD), cache_values.reshape(N_EP, SEQ_DEV, KV_HEADS, LEN, VALUE), lengths.reshape(N_EP, SEQ_DEV))
    attended = lax.map(attend, blocks).reshape(TOKENS, KV_HEADS, group_size, VALUE)
    head_rows = (norm_scale(attended, head_gain.astype(jnp.float32)) * HEAD_SCALE).astype(jnp.bfloat16).reshape(TOKENS, HEADS * VALUE)
    part_width = HEADS * VALUE // N_TP
    attend_out = jnp.zeros((TOKENS, D), jnp.float32)
    for core in range(N_TP):
        head_part = head_rows[:, core * part_width:(core + 1) * part_width]
        attend_out = attend_out + rounded(jnp.dot(head_part, out_proj[core * part_width:(core + 1) * part_width], preferred_element_type=jnp.float32))
    middle = (residual + attend_out).astype(jnp.bfloat16)
    normed_second = norm_scale(middle.astype(jnp.float32), channel_gain.astype(jnp.float32)).astype(jnp.bfloat16)
    dense_gated = jnp.dot(normed_second, dense_gate, preferred_element_type=jnp.float32)
    dense_upper = jnp.dot(normed_second, dense_up, preferred_element_type=jnp.float32)
    dense_hidden = (jax.nn.silu(dense_gated) * dense_upper).astype(jnp.bfloat16)
    dense_out = jnp.dot(dense_hidden, dense_down, preferred_element_type=jnp.float32)
    switch = jax.nn.sigmoid(jnp.dot(normed_second, dense_mixer, preferred_element_type=jnp.float32))
    pair_routes = routes.astype(jnp.int32).reshape(N_EP, SEQ_DEV * TOPK)
    onehot = (pair_routes[..., None] == jnp.arange(EXPERTS).astype(jnp.int32)[None, None, :]).astype(jnp.int32)
    slot_index = lax.optimization_barrier(jnp.sum((jnp.cumsum(onehot, axis=1) - onehot) * onehot, axis=-1)).astype(jnp.int32)
    source_ids = jnp.arange(N_EP).astype(jnp.int32)[:, None]
    placement = (pair_routes * (N_EP * CAP) + source_ids * CAP + slot_index).reshape(TOKENS * TOPK).astype(jnp.int32)
    token_ids = (jnp.arange(TOKENS * TOPK) // TOPK).astype(jnp.int32)
    slot_table = jnp.zeros((EXPERTS * N_EP * CAP,), jnp.int32).at[placement].set(token_ids).reshape(EXPERTS, N_EP * CAP)
    half_units = EXPERT_FF // N_TP

    def run_expert(expert_item):
        row_index, gate_weight, up_weight, down_weight = expert_item
        routed_rows = normed_second[row_index]
        gated = jnp.dot(routed_rows, gate_weight, preferred_element_type=jnp.float32)
        upper = jnp.dot(routed_rows, up_weight, preferred_element_type=jnp.float32)
        hidden = (jax.nn.silu(gated) * upper).astype(jnp.bfloat16)
        output = jnp.zeros((N_EP * CAP, D), jnp.float32)
        for core in range(N_TP):
            output = output + rounded(jnp.dot(hidden[:, core * half_units:(core + 1) * half_units], down_weight[core * half_units:(core + 1) * half_units], preferred_element_type=jnp.float32))
        return output.astype(jnp.bfloat16)
    expert_rows = lax.map(run_expert, (slot_table, expert_gate, expert_up, expert_down))
    picked = expert_rows.reshape(EXPERTS * N_EP * CAP, D)[placement].astype(jnp.float32).reshape(TOKENS, TOPK, D)
    routed = lax.optimization_barrier(jnp.sum(picked * route_weight.astype(jnp.float32)[..., None], axis=1))
    residual_out = (middle.astype(jnp.float32) + routed + switch[:, None] * dense_out).astype(jnp.bfloat16)
    return (residual_out, new_keys.reshape(TOKENS, KV_HEADS, 2 * HEAD), new_values)
```

```python
import jax
import jax.numpy as jnp
from jax import lax
from jax.experimental import pallas as pl
from jax.experimental.pallas import tpu as pltpu
from jax.sharding import PartitionSpec as P

MESH = pl.DeviceIdType.MESH
BF = jnp.bfloat16
F32 = jnp.float32
EPS = 1e-06
NZ, NY, NX = 8, 4, 4
Z_ORDER = (4, 3, 5, 2, 6, 1, 7, 0)
SEQS, WIDTH, LENGTH = 16, 1024, 1024


def norm(rows, gain):
    scale = lax.rsqrt(jnp.mean(rows * rows, axis=-1, keepdims=True) + EPS)
    return rows * scale * gain


def silu(v):
    return v / (1.0 + jnp.exp(-v))


def body(
    residual, attend_gain, channel_gain, mixer, head_gain, cosine, sine,
    lengths, lambdas, routes, routes_turned, route_weight,
    cache_keys, cache_values, w_query, w_key, w_value, w_out,
    e_gate, e_up, e_down, d_gate, d_up, d_down,
    out, new_keys, new_values,
    kbuf, vbuf, wq, wk, wv, wo, egb, eub, edb, dwb,
    qs, kn, nv, att, pa, pb, nsb, sc, snd, rcv, snd2, rcv2, dtok, dps, dpr, fin_s, fin_r,
    load_sem, k_sem, v_sem, own_sem, zs_sem, zr_sem, ps_sem, pr_sem, es_sem, er_sem,
    xs_sem, xr_sem, ms_sem, mr_sem, ts_sem, tr_sem, bs_sem, br_sem, cs_sem, cr_sem,
    fs_sem, fr_sem,
):
    ep = lax.axis_index("ep")
    c = lax.axis_index("tp")
    z = ep // 16
    y = (ep // 4) % 4
    x = ep % 4
    parity = x % 2
    me = z * 8 + y * 2 + x // 2
    self_in = parity == c
    other = (ep, 1 - c)

    def partner(n):
        return ((n // 8) * 16 + ((n // 2) % 4) * 4 + (n % 2) * 2 + c, parity)

    def is_self(n):
        return jnp.logical_and(self_in, n == me)

    def z_peer(d):
        return (((z + d) % NZ) * 16 + y * 4 + x, c)

    def near(zz, k):
        return zz * 8 + ((y + k // 2) % 4) * 2 + (x // 2 + k % 2) % 2

    barrier = pltpu.get_barrier_semaphore()
    for dz in Z_ORDER:
        zz = (z + dz) % NZ

        @pl.loop(0, 8)
        def _(k):
            n = near(zz, 7 - k)

            @pl.when(jnp.logical_not(is_self(n)))
            def _():
                pl.semaphore_signal(barrier, inc=1, device_id=partner(n), device_id_type=MESH)

    for d in range(1, 8):
        pl.semaphore_signal(barrier, inc=1, device_id=z_peer(d), device_id_type=MESH)
    pl.semaphore_signal(barrier, inc=1, device_id=other, device_id_type=MESH)

    loads = [
        pltpu.make_async_copy(src, dst, load_sem.at[i])
        for i, (src, dst) in enumerate(
            [(w_query, wq), (w_key, wk), (w_value, wv), (w_out, wo),
             (e_gate, egb.at[c]), (e_up, eub.at[c]), (e_down, edb.at[c])]
        )
    ]
    own_parts = [
        pltpu.make_async_copy(src, dwb.at[z, c, i], own_sem.at[i])
        for i, src in enumerate([d_gate, d_up, d_down])
    ]
    kv = [
        (
            pltpu.make_async_copy(cache_keys.at[s], kbuf.at[s], k_sem.at[s]),
            pltpu.make_async_copy(cache_values.at[s], vbuf.at[s], v_sem.at[s]),
        )
        for s in range(SEQS)
    ]
    for i in range(3):
        loads[i].start()
    for cp in own_parts:
        cp.start()
    for s in range(SEQS):
        kv[s][0].start()
        kv[s][1].start()
    for i in range(3, 7):
        loads[i].start()

    row128 = lax.broadcasted_iota(jnp.int32, (128, SEQS), 0)
    expert_t = (row128 // 2) * 2 + c
    hit_t = jnp.zeros((128, SEQS), F32)
    for k in range(6):
        hit_t = hit_t + jnp.where(routes_turned[k : k + 1, :] == expert_t, 1.0, 0.0)
    up_tri = jnp.where(
        lax.broadcasted_iota(jnp.int32, (SEQS, SEQS), 0)
        < lax.broadcasted_iota(jnp.int32, (SEQS, SEQS), 1),
        1.0, 0.0,
    )
    rank_t = jnp.dot(hit_t.astype(BF), up_tri.astype(BF), preferred_element_type=F32)
    pick_t = jnp.where(rank_t == (row128 % 2).astype(F32), hit_t, 0.0).astype(BF)

    lane128 = lax.broadcasted_iota(jnp.int32, (SEQS, 128), 1)
    expert_l = (lane128 // 2) * 2 + c
    hit_l = jnp.zeros((SEQS, 128), F32)
    weight_l = jnp.zeros((SEQS, 128), F32)
    for k in range(6):
        same = routes[:, k : k + 1] == expert_l
        hit_l = hit_l + jnp.where(same, 1.0, 0.0)
        weight_l = weight_l + jnp.where(same, route_weight[:, k : k + 1], 0.0)
    low_tri = jnp.where(
        lax.broadcasted_iota(jnp.int32, (SEQS, SEQS), 1)
        < lax.broadcasted_iota(jnp.int32, (SEQS, SEQS), 0),
        1.0, 0.0,
    )
    rank_l = jnp.dot(low_tri.astype(BF), hit_l.astype(BF), preferred_element_type=F32)
    combine = jnp.where(rank_l == (lane128 % 2).astype(F32), weight_l, 0.0)
    c_hi = combine.astype(BF)
    rest = combine - c_hi.astype(F32)
    c_mid = rest.astype(BF)
    c_lo = (rest - c_mid.astype(F32)).astype(BF)
    combine3 = jnp.concatenate([c_hi, c_mid, c_lo], axis=0)

    res = residual[...].astype(F32)
    normed = norm(res, attend_gain[...].astype(F32)).astype(BF)
    for i in range(3):
        loads[i].wait()
    q = jnp.dot(normed, wq[...], preferred_element_type=F32)
    kk = jnp.dot(normed, wk[...], preferred_element_type=F32)
    vv = jnp.dot(normed, wv[...], preferred_element_type=F32).astype(BF)
    cos_t, sin_t = cosine[...], sine[...]
    first = (lane128 % 64) < 32

    def rotated(u):
        swapped = jnp.where(first, pltpu.roll(u, 96, 1), pltpu.roll(u, 32, 1))
        return (u * cos_t + swapped * sin_t).astype(BF)

    k_rot = rotated(kk)
    new_keys[...] = k_rot
    new_values[...] = vv
    kn[...] = k_rot.astype(F32)
    nv[...] = vv.astype(F32)
    qs[...] = jnp.zeros((SEQS, 8, 128), F32)
    for g in range(2):
        q_rot = rotated(q[:, 128 * g : 128 * g + 128]).astype(F32) * 0.125
        qs[:, g, :] = jnp.where(lane128 < 64, q_rot, 0.0)
        qs[:, 4 + g, :] = jnp.where(lane128 < 64, 0.0, q_rot)

    sub8 = lax.broadcasted_iota(jnp.int32, (8, 1), 0)
    lam = jnp.where(sub8 == 0, lambdas[0], lambdas[1])
    position = lax.broadcasted_iota(jnp.int32, (8, LENGTH), 1)

    def attend(s):
        kv[s][0].wait()
        query = qs[s]
        scores = lax.dot_general(
            query.astype(BF), kbuf[s], (((1,), (1,)), ((), ())), preferred_element_type=F32
        )
        e = jnp.where(position < lengths[s], jnp.exp(scores), 0.0)
        own = jnp.exp(
            jnp.broadcast_to(jnp.sum(query * kn[s : s + 1, :], axis=-1, keepdims=True), (8, 128))
        )
        inverse = 1.0 / (jnp.sum(e, axis=-1, keepdims=True) + own)
        p = e * inverse[:, 0:1]
        po = own * inverse
        w = (p - lam * pltpu.roll(p, 4, 0)).astype(BF)
        w_own = (po - lam * pltpu.roll(po, 4, 0)).astype(BF).astype(F32)
        kv[s][1].wait()
        att[s] = jnp.dot(w, vbuf[s], preferred_element_type=F32) + w_own * nv[s : s + 1, :]

    for s in range(8):
        attend(s)

    pl.semaphore_wait(barrier, 64 + 7 + 1 - self_in.astype(jnp.int32))

    def z_copy(src, d_at_dest, hop, part=None):
        ref = dwb.at[src, c] if part is None else dwb.at[src, c, part]
        return pltpu.make_async_remote_copy(
            src_ref=ref, dst_ref=ref, send_sem=zs_sem.at[d_at_dest if part is None else 8 + part.start // 2],
            recv_sem=zr_sem.at[d_at_dest if part is None else 8 + part.start // 2],
            device_id=z_peer(hop), device_id_type=MESH,
        )

    for cp in own_parts:
        cp.wait()
    step1 = [z_copy(z, (-h) % 8, h) for h in (2, -2, 1, -1)]
    for cp in step1:
        cp.start()
    swaps = [
        pltpu.make_async_remote_copy(
            src_ref=src, dst_ref=dst.at[c], send_sem=es_sem.at[i], recv_sem=er_sem.at[i],
            device_id=other, device_id_type=MESH,
        )
        for i, (src, dst) in enumerate([(e_gate, egb), (e_up, eub), (e_down, edb)])
    ]
    for cp in swaps:
        cp.start()

    for s in range(8, SEQS):
        attend(s)

    gain_h = head_gain[...].astype(F32)
    rows = jnp.concatenate(
        [(norm(att[:, g, :], gain_h) * 0.8).astype(BF) for g in range(2)], axis=1
    )
    loads[3].wait()
    pa[...] = jnp.dot(rows, wo[...], preferred_element_type=F32).astype(BF)
    swap_a = pltpu.make_async_remote_copy(
        src_ref=pa, dst_ref=pb, send_sem=xs_sem, recv_sem=xr_sem,
        device_id=other, device_id_type=MESH,
    )
    swap_a.start()
    swap_a.wait()
    middle = (res + (pa[...].astype(F32) + pb[...].astype(F32))).astype(BF).astype(F32)
    ns = norm(middle, channel_gain[...].astype(F32)).astype(BF)
    nsb[...] = ns
    switch = jax.nn.sigmoid(
        jnp.sum(ns.astype(F32) * mixer[...].astype(F32), axis=-1, keepdims=True)
    )

    def spread(values):
        for j in range(8):
            sc[pl.ds(j, 128, stride=8), :] = values[:, 128 * j : 128 * j + 128]

    def send_blocks(src, dst, send_sem, recv_sem):
        for dz in Z_ORDER:
            zz = (z + dz) % NZ

            @pl.loop(0, 8)
            def _(k):
                n = near(zz, 7 - k)

                @pl.when(is_self(n))
                def _():
                    pltpu.make_async_copy(src.at[n], dst.at[me], recv_sem.at[z]).start()

                @pl.when(jnp.logical_not(is_self(n)))
                def _():
                    pltpu.make_async_remote_copy(
                        src_ref=src.at[n], dst_ref=dst.at[me], send_sem=send_sem,
                        recv_sem=recv_sem.at[z], device_id=partner(n), device_id_type=MESH,
                    ).start()

    def sent_all(buf, send_sem, count):
        @pl.when(self_in)
        def _():
            part = buf.at[pl.ds(0, count - 1)]
            pltpu.make_async_copy(part, part, send_sem).wait()

        @pl.when(jnp.logical_not(self_in))
        def _():
            pltpu.make_async_copy(buf, buf, send_sem).wait()

    def send_plane(pick_src, dst, send_sem, recv_sem):
        @pl.loop(0, 8)
        def _(k):
            n = near(z, 7 - k)
            src = pick_src(n % 8)

            @pl.when(is_self(n))
            def _():
                pltpu.make_async_copy(src, dst.at[me % 8], recv_sem).start()

            @pl.when(jnp.logical_not(is_self(n)))
            def _():
                pltpu.make_async_remote_copy(
                    src_ref=src, dst_ref=dst.at[me % 8], send_sem=send_sem,
                    recv_sem=recv_sem, device_id=partner(n), device_id_type=MESH,
                ).start()

    spread(jnp.dot(pick_t, ns, preferred_element_type=F32))
    snd[...] = sc[...].reshape(64, 16, 128).astype(BF)
    send_blocks(snd, rcv, ms_sem, mr_sem)
    send_plane(lambda n: nsb, dtok, ts_sem, tr_sem)

    for d in (7, 6, 1, 2):
        src = (z + d) % NZ
        pltpu.make_async_copy(dwb.at[src, c], dwb.at[src, c], zr_sem.at[d]).wait()
    step2 = [
        z_copy((z + 2) % 8, 4, -2, pl.ds(0, 2)),
        z_copy((z - 2) % 8, 4, 2, pl.ds(2, 1)),
        z_copy((z + 2) % 8, 3, -1),
        z_copy((z - 2) % 8, 5, 1),
    ]
    for cp in step2:
        cp.start()

    def forward(d):
        ref = dwb.at[(z + d) % NZ, c]
        return pltpu.make_async_remote_copy(
            src_ref=ref, dst_ref=ref, send_sem=ps_sem.at[d], recv_sem=pr_sem.at[d],
            device_id=other, device_id_type=MESH,
        )

    for d in (0, 1, 7, 2, 6):
        forward(d).start()

    for i in range(4, 7):
        loads[i].wait()
    for cp in swaps:
        cp.wait()
    for zz in range(8):
        part = rcv.at[pl.ds(zz * 8, 8)]
        pltpu.make_async_copy(part, part, mr_sem.at[zz]).wait()
    sc[...] = rcv[...].reshape(1024, 128).astype(F32)

    def gathered():
        return jnp.concatenate(
            [sc[pl.ds(j, 128, stride=8), :].astype(BF) for j in range(8)], axis=1
        )

    xr = gathered()
    total = jnp.zeros((128, WIDTH), F32)
    for h in range(2):
        gate = jnp.dot(xr, egb[h], preferred_element_type=F32)
        upper = jnp.dot(xr, eub[h], preferred_element_type=F32)
        hidden = (silu(gate) * upper).astype(BF)
        total = total + jnp.dot(hidden, edb[h], preferred_element_type=F32).astype(BF).astype(F32)
    spread(total)
    snd2[...] = sc[...].reshape(64, 16, 128).astype(BF)
    send_blocks(snd2, rcv2, bs_sem, br_sem)

    for d in (3, 5):
        src = (z + d) % NZ
        pltpu.make_async_copy(dwb.at[src, c], dwb.at[src, c], zr_sem.at[d]).wait()
    far = dwb.at[(z + 4) % NZ, c]
    for i, part in enumerate((far.at[pl.ds(0, 2)], far.at[pl.ds(2, 1)])):
        pltpu.make_async_copy(part, part, zr_sem.at[8 + i]).wait()
    for d in (3, 5, 4):
        forward(d).start()
    pltpu.make_async_copy(dtok, dtok, tr_sem).wait()
    for d in range(8):
        mirror = dwb.at[(z + d) % NZ, 1 - c]
        pltpu.make_async_copy(mirror, mirror, pr_sem.at[d]).wait()
    xd = dtok[...].reshape(128, WIDTH)
    turned = (((1,), (1,)), ((), ()))
    gate_w = dwb[:, :, 0].reshape(256, WIDTH)
    up_w = dwb[:, :, 1].reshape(256, WIDTH)
    down_w = dwb[:, :, 2].reshape(256, WIDTH)
    gate = lax.dot_general(xd, gate_w, turned, preferred_element_type=F32)
    upper = lax.dot_general(xd, up_w, turned, preferred_element_type=F32)
    hidden = (silu(gate) * upper).astype(BF)
    dps[...] = jnp.dot(hidden, down_w, preferred_element_type=F32).astype(BF).reshape(8, 16, WIDTH)
    send_plane(lambda n: dps.at[n], dpr, cs_sem, cr_sem)

    for zz in range(8):
        part = rcv2.at[pl.ds(zz * 8, 8)]
        pltpu.make_async_copy(part, part, br_sem.at[zz]).wait()
    sc[...] = rcv2[...].reshape(1024, 128).astype(F32)
    three = jnp.dot(combine3, gathered(), preferred_element_type=F32)
    routed = three[0:16] + (three[16:32] + three[32:48])
    pltpu.make_async_copy(dpr, dpr, cr_sem).wait()
    dense = dpr[0].astype(F32)
    for i in range(1, 8):
        dense = dense + dpr[i].astype(F32)
    fin_s[...] = routed + switch * dense
    swap_f = pltpu.make_async_remote_copy(
        src_ref=fin_s, dst_ref=fin_r, send_sem=fs_sem, recv_sem=fr_sem,
        device_id=other, device_id_type=MESH,
    )
    swap_f.start()
    sent_all(snd, ms_sem, 64)
    sent_all(snd2, bs_sem, 64)
    sent_all(dtok, ts_sem, 8)
    sent_all(dps, cs_sem, 8)
    for cp in step1 + step2:
        cp.wait_send()
    for d in range(8):
        forward(d).wait_send()
    swap_f.wait()
    out[...] = (middle + (fin_s[...] + fin_r[...])).astype(BF)


def per_device(
    residual_in, lengths, cache_keys, cache_values, attend_gain, query_proj, key_proj,
    value_proj, lambdas, head_gain, out_proj, channel_gain, routes, route_weight,
    expert_gate, expert_up, expert_down, dense_gate, dense_up, dense_down, dense_mixer,
):
    inverse = 10000.0 ** (-jnp.arange(32, dtype=F32) / 32)
    angles = lengths.astype(F32)[:, None] * inverse
    cos, sin = jnp.cos(angles), jnp.sin(angles)
    cosine = jnp.concatenate([cos, cos, cos, cos], axis=1)
    sine = jnp.concatenate([-sin, sin, -sin, sin], axis=1)
    vm = pl.BlockSpec(memory_space=pltpu.VMEM)
    sm = pl.BlockSpec(memory_space=pltpu.SMEM)
    hb = pl.BlockSpec(memory_space=pl.ANY)
    DMA = pltpu.SemaphoreType.DMA
    V = pltpu.VMEM
    out, keys, values = pl.pallas_call(
        body,
        name="layer",
        out_shape=(
            jax.ShapeDtypeStruct((SEQS, WIDTH), BF),
            jax.ShapeDtypeStruct((SEQS, 128), BF),
            jax.ShapeDtypeStruct((SEQS, 128), BF),
        ),
        in_specs=[vm] * 7 + [sm] * 2 + [vm] * 3 + [hb] * 12,
        out_specs=(vm, vm, vm),
        scratch_shapes=[
            V((SEQS, LENGTH, 128), BF), V((SEQS, LENGTH, 128), BF),
            V((1024, 256), BF), V((1024, 128), BF), V((1024, 128), BF), V((256, 1024), BF),
            V((2, 1024, 256), BF), V((2, 1024, 256), BF), V((2, 256, 1024), BF),
            V((8, 2, 3, 16, 1024), BF),
            V((SEQS, 8, 128), F32), V((SEQS, 128), F32), V((SEQS, 128), F32),
            V((SEQS, 8, 128), F32),
            V((SEQS, WIDTH), BF), V((SEQS, WIDTH), BF), V((SEQS, WIDTH), BF),
            V((1024, 128), F32),
            V((64, 16, 128), BF), V((64, 16, 128), BF), V((64, 16, 128), BF), V((64, 16, 128), BF),
            V((8, 16, WIDTH), BF), V((8, 16, WIDTH), BF), V((8, 16, WIDTH), BF),
            V((SEQS, WIDTH), F32), V((SEQS, WIDTH), F32),
            DMA((7,)), DMA((16,)), DMA((16,)), DMA((3,)),
            DMA((10,)), DMA((10,)), DMA((8,)), DMA((8,)), DMA((3,)), DMA((3,)),
            DMA, DMA, DMA, DMA((8,)), DMA, DMA, DMA, DMA((8,)), DMA, DMA,
            DMA, DMA,
        ],
        compiler_params=pltpu.CompilerParams(
            collective_id=0, has_side_effects=True, vmem_limit_bytes=60 * 1024 * 1024
        ),
    )(
        residual_in, attend_gain.reshape(1, -1), channel_gain.reshape(1, -1),
        dense_mixer.reshape(1, -1), head_gain.reshape(1, -1), cosine, sine,
        lengths, lambdas, routes, routes.T, route_weight,
        cache_keys.reshape(SEQS, LENGTH, 128), cache_values.reshape(SEQS, LENGTH, 128),
        query_proj, key_proj, value_proj, out_proj,
        expert_gate[0], expert_up[0], expert_down[0], dense_gate.T, dense_up.T, dense_down,
    )
    return out, keys.reshape(SEQS, 1, 128), values.reshape(SEQS, 1, 128)


def solution(mesh):
    placed = (
        P("ep", None), P("ep"), P("ep", "tp", None, None), P("ep", "tp", None, None), P(),
        P(None, "tp"), P(None, "tp"), P(None, "tp"), P("tp"), P(), P("tp", None), P(),
        P("ep", None), P("ep", None), P("ep", None, "tp"), P("ep", None, "tp"),
        P("ep", "tp", None), P(None, ("ep", "tp")), P(None, ("ep", "tp")),
        P(("ep", "tp"), None), P(),
    )
    return jax.shard_map(
        per_device, mesh=mesh, in_specs=placed,
        out_specs=(P("ep", None), P("ep", "tp", None), P("ep", "tp", None)),
        check_vma=False,
    )
```

```python
import jax
import jax.numpy as jnp
import numpy as np
from jax import lax
from jax.experimental import pallas as pl
from jax.experimental.pallas import tpu as pltpu
from jax.sharding import PartitionSpec as P

MESH = pl.DeviceIdType.MESH
BF = jnp.bfloat16
F32 = jnp.float32
EPS = 1e-06
NZ, NY, NX = 8, 4, 4
SEQS, WIDTH, LENGTH = 16, 1024, 1024


def norm(rows, gain):
    scale = lax.rsqrt(jnp.mean(rows * rows, axis=-1, keepdims=True) + EPS)
    return rows * scale * gain


def silu(v):
    return v / (1.0 + jnp.exp(-v))


def body(
    residual, attend_gain, channel_gain, mixer, head_gain, frequency,
    lengths, lambdas, routes_turned, weight_turned,
    cache_keys, cache_values, w_query, w_key, w_value, w_out,
    e_gate, e_up, e_down, d_gate, d_up, d_down,
    out, new_keys, new_values,
    kbuf, vbuf, wq, wk, wv, wo, egb, eub, edb, dwb,
    qs, kn, nv, att, pa, pb, nsb, sc, snd, rcv, snd2, rcv2, dtok, dps, dpr, fin_s, fin_r,
    load_sem, k_sem, v_sem, own_sem, zs_sem, zr_sem, ps_sem, pr_sem, es_sem, er_sem,
    xs_sem, xr_sem, ms_sem, mr_sem, ts_sem, tr_sem, bs_sem, br_sem, cs_sem, cr_sem,
    fs_sem, fr_sem, line_sem,
):
    ep = lax.axis_index("ep")
    c = lax.axis_index("tp")
    z = ep // 16
    y = (ep // 4) % 4
    x = ep % 4
    parity = x % 2
    me = z * 8 + y * 2 + x // 2
    self_in = parity == c
    other = (ep, 1 - c)

    plane = []
    for k in range(8):
        yy = (y + 3 - k // 2) % 4
        xh = (x // 2 + 1 - k % 2) % 2
        plane.append((yy * 4 + xh * 2 + c, yy * 2 + xh))
    mine = me % 8

    def z_peer(d):
        return (((z + d) % NZ) * 16 + y * 4 + x, c)

    loads = [
        pltpu.make_async_copy(src, dst, load_sem.at[i])
        for i, (src, dst) in enumerate(
            [(w_query, wq), (w_key, wk), (w_value, wv), (w_out, wo),
             (e_gate, egb.at[c]), (e_up, eub.at[c]), (e_down, edb.at[c])]
        )
    ]
    own_parts = [
        pltpu.make_async_copy(src, dwb.at[z, c, i], own_sem.at[i])
        for i, src in enumerate([d_gate, d_up, d_down])
    ]
    kv = [
        (
            pltpu.make_async_copy(cache_keys.at[s], kbuf.at[s], k_sem.at[s]),
            pltpu.make_async_copy(cache_values.at[s], vbuf.at[s], v_sem.at[s]),
        )
        for s in range(SEQS)
    ]
    for cp in own_parts:
        cp.start()
    for i in range(3):
        loads[i].start()

    def stream(sequences):
        for kind in range(2):
            for s in sequences:
                kv[s][kind].start()

    stream(range(8))

    barrier = pltpu.get_barrier_semaphore()
    for d in (4, 3, 5, 2, 6, 1, 7):
        pl.semaphore_signal(barrier, inc=1, device_id=z_peer(d), device_id_type=MESH)
    for chip, slot in plane:

        @pl.when(jnp.logical_not(jnp.logical_and(self_in, slot == mine)))
        def _(chip=chip):
            pl.semaphore_signal(barrier, inc=1, device_id=(z * 16 + chip, parity), device_id_type=MESH)

    pl.semaphore_signal(barrier, inc=1, device_id=other, device_id_type=MESH)

    row128 = lax.broadcasted_iota(jnp.int32, (128, SEQS), 0)
    expert_t = (row128 // 2) * 2 + c
    hit_t = jnp.zeros((128, SEQS), F32)
    weight_t = jnp.zeros((128, SEQS), F32)
    for k in range(6):
        same = routes_turned[k : k + 1, :] == expert_t
        hit_t = hit_t + jnp.where(same, 1.0, 0.0)
        weight_t = weight_t + jnp.where(same, weight_turned[k : k + 1, :], 0.0)
    up_tri = jnp.where(
        lax.broadcasted_iota(jnp.int32, (SEQS, SEQS), 0)
        < lax.broadcasted_iota(jnp.int32, (SEQS, SEQS), 1),
        1.0, 0.0,
    )
    rank_t = jnp.dot(hit_t.astype(BF), up_tri.astype(BF), preferred_element_type=F32)
    pick_t = jnp.where(rank_t == (row128 % 2).astype(F32), hit_t, 0.0).astype(BF)

    combine_t = jnp.where(rank_t == (row128 % 2).astype(F32), weight_t, 0.0)
    c_hi = combine_t.astype(BF)
    rest = combine_t - c_hi.astype(F32)
    c_mid = rest.astype(BF)
    c_lo = (rest - c_mid.astype(F32)).astype(BF)
    eye = jnp.where(
        lax.broadcasted_iota(jnp.int32, (SEQS, SEQS), 0)
        == lax.broadcasted_iota(jnp.int32, (SEQS, SEQS), 1),
        1.0, 0.0,
    ).astype(BF)
    combine3 = jnp.concatenate(
        [
            lax.dot_general(eye, part, (((1,), (1,)), ((), ())), preferred_element_type=F32)
            for part in (c_hi, c_mid, c_lo)
        ],
        axis=0,
    ).astype(BF)

    stream(range(8, SEQS))
    loads[3].start()

    res = residual[...].astype(F32)
    normed = norm(res, attend_gain[...].astype(F32).reshape(1, WIDTH)).astype(BF)
    for i in range(3):
        loads[i].wait()
    q = jnp.dot(normed, wq[...], preferred_element_type=F32)
    kk = jnp.dot(normed, wk[...], preferred_element_type=F32)
    vv = jnp.dot(normed, wv[...], preferred_element_type=F32).astype(BF)
    lane128 = lax.broadcasted_iota(jnp.int32, (SEQS, 128), 1)
    row16 = lax.broadcasted_iota(jnp.int32, (SEQS, 128), 0)
    first = (lane128 % 64) < 32
    place = jnp.zeros((SEQS, 128), jnp.int32)
    for s in range(SEQS):
        place = jnp.where(row16 == s, lengths[s], place)
    angles = place.astype(F32) * frequency[...]
    cos_t, sin_t = jnp.cos(angles), jnp.sin(angles)
    sin_t = jnp.where(first, -sin_t, sin_t)

    def rotated(u):
        swapped = jnp.where(first, pltpu.roll(u, 96, 1), pltpu.roll(u, 32, 1))
        return (u * cos_t + swapped * sin_t).astype(BF)

    k_rot = rotated(kk)
    new_keys[...] = k_rot
    new_values[...] = vv
    kn[...] = k_rot.astype(F32)
    nv[...] = vv.astype(F32)
    for g in range(2):
        q_rot = rotated(q[:, 128 * g : 128 * g + 128]).astype(F32) * 0.125
        qs[pl.ds(g, SEQS, stride=4), :] = jnp.where(lane128 < 64, q_rot, 0.0)
        qs[pl.ds(2 + g, SEQS, stride=4), :] = jnp.where(lane128 < 64, 0.0, q_rot)

    pl.semaphore_wait(barrier, 7 + 8 + 1 - self_in.astype(jnp.int32))
    for d in (4, 3, 5, 2, 6, 1, 7):
        pl.semaphore_signal(line_sem, inc=1, device_id=z_peer(d), device_id_type=MESH)

    def z_copy(d, hop):
        ref = dwb.at[(z + hop + d) % NZ, c]
        return pltpu.make_async_remote_copy(
            src_ref=ref, dst_ref=ref, send_sem=zs_sem.at[d], recv_sem=zr_sem.at[d],
            device_id=z_peer(hop), device_id_type=MESH,
        )

    def z_wait(d):
        ref = dwb.at[(z + d) % NZ, c]
        pltpu.make_async_copy(ref, ref, zr_sem.at[d % NZ]).wait()

    def forward(d):
        ref = dwb.at[(z + d) % NZ, c]
        return pltpu.make_async_remote_copy(
            src_ref=ref, dst_ref=ref, send_sem=ps_sem.at[d], recv_sem=pr_sem.at[d],
            device_id=other, device_id_type=MESH,
        )

    for cp in own_parts:
        cp.wait()
    step1 = [z_copy(4, 4), z_copy(7, 1), z_copy(1, -1)]
    for cp in step1:
        cp.start()
    swaps = [
        pltpu.make_async_remote_copy(
            src_ref=src, dst_ref=dst.at[c], send_sem=es_sem.at[i], recv_sem=er_sem.at[i],
            device_id=other, device_id_type=MESH,
        )
        for i, (src, dst) in enumerate([(e_gate, egb), (e_up, eub), (e_down, edb)])
    ]
    forward(0).start()

    sub8 = lax.broadcasted_iota(jnp.int32, (8, 1), 0)
    low8 = sub8 < 4
    lam = jnp.where(sub8 % 2 == 0, lambdas[0], lambdas[1])
    position = lax.broadcasted_iota(jnp.int32, (8, LENGTH), 1)
    turned = (((1,), (1,)), ((), ()))

    def attend(pairs):
        for p in pairs:
            kv[2 * p][0].wait()
            kv[2 * p + 1][0].wait()
        scores, own = [], []
        for p in pairs:
            query = qs[8 * p : 8 * p + 8, :]
            first_q = jnp.where(low8, query, 0.0).astype(BF)
            second_q = jnp.where(low8, 0.0, query).astype(BF)
            scores.append(
                lax.dot_general(first_q, kbuf[2 * p], turned, preferred_element_type=F32)
                + lax.dot_general(second_q, kbuf[2 * p + 1], turned, preferred_element_type=F32)
            )
            key = jnp.where(low8, kn[2 * p : 2 * p + 1, :], kn[2 * p + 1 : 2 * p + 2, :])
            own.append(
                jnp.exp(jnp.broadcast_to(jnp.sum(query * key, axis=-1, keepdims=True), (8, 128)))
            )
        weights, own_weights = [], []
        for i, p in enumerate(pairs):
            limit = jnp.where(low8, lengths[2 * p], lengths[2 * p + 1])
            e = jnp.where(position < limit, jnp.exp(scores[i]), 0.0)
            inverse = 1.0 / (jnp.sum(e, axis=-1, keepdims=True) + own[i])
            share = e * inverse[:, 0:1]
            share_own = own[i] * inverse
            weights.append((share - lam * pltpu.roll(share, 6, 0)).astype(BF))
            own_weights.append(
                (share_own - lam * pltpu.roll(share_own, 6, 0)).astype(BF).astype(F32)
            )
        for p in pairs:
            kv[2 * p][1].wait()
            kv[2 * p + 1][1].wait()
        for i, p in enumerate(pairs):
            first_a = jnp.dot(weights[i], vbuf[2 * p], preferred_element_type=F32)
            second_a = jnp.dot(weights[i], vbuf[2 * p + 1], preferred_element_type=F32)
            value = jnp.where(low8, nv[2 * p : 2 * p + 1, :], nv[2 * p + 1 : 2 * p + 2, :])
            att[8 * p : 8 * p + 8, :] = (
                jnp.where(low8, first_a, second_a) + own_weights[i] * value
            )

    attend((0, 1, 2, 3))
    for i in range(4, 7):
        loads[i].start()

    attend((4, 5, 6, 7))

    gain_h = head_gain[...].astype(F32).reshape(1, 128)
    rows = jnp.concatenate(
        [(norm(att[pl.ds(g, SEQS, stride=4), :], gain_h) * 0.8).astype(BF) for g in range(2)], axis=1
    )
    loads[3].wait()
    pa[...] = jnp.dot(rows, wo[...], preferred_element_type=F32).astype(BF)
    swap_a = pltpu.make_async_remote_copy(
        src_ref=pa, dst_ref=pb, send_sem=xs_sem, recv_sem=xr_sem,
        device_id=other, device_id_type=MESH,
    )
    swap_a.start()
    for cp in swaps:
        cp.start()
    swap_a.wait()
    middle = (res + (pa[...].astype(F32) + pb[...].astype(F32))).astype(BF).astype(F32)
    ns = norm(middle, channel_gain[...].astype(F32).reshape(1, WIDTH)).astype(BF)
    nsb[...] = ns
    switch = jax.nn.sigmoid(
        jnp.sum(ns.astype(F32) * mixer[...].astype(F32).reshape(1, WIDTH), axis=-1, keepdims=True)
    )

    def spread(values):
        for j in range(8):
            sc[pl.ds(j, 128, stride=8), :] = values[:, 128 * j : 128 * j + 128]

    def send_blocks(src, dst, send_sem, recv_sem, distances):
        for dz in distances:
            zz = (z + dz) % NZ
            for chip, slot in plane:
                n = zz * 8 + slot
                remote = pltpu.make_async_remote_copy(
                    src_ref=src.at[n], dst_ref=dst.at[me], send_sem=send_sem,
                    recv_sem=recv_sem.at[z], device_id=(zz * 16 + chip, parity),
                    device_id_type=MESH,
                )
                if dz:
                    remote.start()
                    continue
                self_block = jnp.logical_and(self_in, slot == mine)

                @pl.when(self_block)
                def _(n=n):
                    pltpu.make_async_copy(src.at[n], dst.at[me], recv_sem.at[z]).start()

                @pl.when(jnp.logical_not(self_block))
                def _(remote=remote):
                    remote.start()

    def sent_all(buf, send_sem, count):
        @pl.when(self_in)
        def _():
            part = buf.at[pl.ds(0, count - 1)]
            pltpu.make_async_copy(part, part, send_sem).wait()

        @pl.when(jnp.logical_not(self_in))
        def _():
            pltpu.make_async_copy(buf, buf, send_sem).wait()

    def send_plane(pick_src, dst, send_sem, recv_sem):
        for chip, slot in plane:
            src = pick_src(slot)
            self_block = jnp.logical_and(self_in, slot == mine)

            @pl.when(self_block)
            def _(src=src):
                pltpu.make_async_copy(src, dst.at[mine], recv_sem).start()

            @pl.when(jnp.logical_not(self_block))
            def _(src=src, chip=chip):
                pltpu.make_async_remote_copy(
                    src_ref=src, dst_ref=dst.at[mine], send_sem=send_sem,
                    recv_sem=recv_sem, device_id=(z * 16 + chip, parity), device_id_type=MESH,
                ).start()

    picked = jnp.dot(pick_t, ns, preferred_element_type=F32)
    for j in range(8):
        sc[pl.ds(j, 128, stride=8), :] = picked[:, 128 * j : 128 * j + 128]
    snd[...] = sc[...].reshape(64, 16, 128).astype(BF)
    pl.semaphore_wait(line_sem, 7)
    send_blocks(snd, rcv, ms_sem, mr_sem, (4, 3, 5, 2, 6, 1, 7, 0))
    send_plane(lambda n: nsb, dtok, ts_sem, tr_sem)

    for d in (7, 1, 4):
        z_wait(d)
    step2 = [z_copy(6, 1), z_copy(2, -1), z_copy(3, 1), z_copy(5, -1)]
    for cp in step2:
        cp.start()
    for d in (1, 7, 4):
        forward(d).start()

    for i in range(4, 7):
        loads[i].wait()
    for cp in swaps:
        cp.wait()

    def serve(distances):
        count = len(distances)
        slots = [pl.ds(((z + d) % NZ) * 8, 8) for d in distances]
        for d, part in zip(distances, slots):
            ref = rcv.at[part]
            pltpu.make_async_copy(ref, ref, mr_sem.at[(z + d) % NZ]).wait()
        for i, part in enumerate(slots):
            sc[128 * i : 128 * i + 128, :] = rcv[part].reshape(128, 128).astype(F32)
        rows = jnp.concatenate(
            [sc[pl.ds(j, 16 * count, stride=8), :].astype(BF) for j in range(8)], axis=1
        )
        total = None
        for h in range(2):
            gate = jnp.dot(rows, egb[h], preferred_element_type=F32)
            upper = jnp.dot(rows, eub[h], preferred_element_type=F32)
            hidden = (silu(gate) * upper).astype(BF)
            half = jnp.dot(hidden, edb[h], preferred_element_type=F32).astype(BF).astype(F32)
            total = half if total is None else total + half
        for j in range(8):
            sc[pl.ds(j, 16 * count, stride=8), :] = total[:, 128 * j : 128 * j + 128]
        for i, part in enumerate(slots):
            snd2[part] = sc[128 * i : 128 * i + 128, :].reshape(8, 16, 128).astype(BF)
        send_blocks(snd2, rcv2, bs_sem, br_sem, distances)

    serve((4, 3, 5, 2, 6, 1, 7, 0))

    for d in (2, 6, 3, 5):
        z_wait(d)
        forward(d).start()
    pltpu.make_async_copy(dtok, dtok, tr_sem).wait()
    for d in range(8):
        mirror = dwb.at[(z + d) % NZ, 1 - c]
        pltpu.make_async_copy(mirror, mirror, pr_sem.at[d]).wait()
    xd = dtok[...].reshape(128, WIDTH)
    gate_w = dwb[:, :, 0].reshape(256, WIDTH)
    up_w = dwb[:, :, 1].reshape(256, WIDTH)
    down_w = dwb[:, :, 2].reshape(256, WIDTH)
    gate = lax.dot_general(xd, gate_w, turned, preferred_element_type=F32)
    upper = lax.dot_general(xd, up_w, turned, preferred_element_type=F32)
    hidden = (silu(gate) * upper).astype(BF)
    dps[...] = jnp.dot(hidden, down_w, preferred_element_type=F32).astype(BF).reshape(8, 16, WIDTH)
    send_plane(lambda n: dps.at[n], dpr, cs_sem, cr_sem)

    for zz in range(8):
        part = rcv2.at[pl.ds(zz * 8, 8)]
        pltpu.make_async_copy(part, part, br_sem.at[zz]).wait()
    sc[...] = rcv2[...].reshape(1024, 128).astype(F32)
    returned = jnp.concatenate(
        [sc[pl.ds(j, 128, stride=8), :].astype(BF) for j in range(8)], axis=1
    )
    three = jnp.dot(combine3, returned, preferred_element_type=F32)
    routed = three[0:16] + (three[16:32] + three[32:48])
    pltpu.make_async_copy(dpr, dpr, cr_sem).wait()
    dense = dpr[0].astype(F32)
    for i in range(1, 8):
        dense = dense + dpr[i].astype(F32)
    fin_s[...] = routed + switch * dense
    swap_f = pltpu.make_async_remote_copy(
        src_ref=fin_s, dst_ref=fin_r, send_sem=fs_sem, recv_sem=fr_sem,
        device_id=other, device_id_type=MESH,
    )
    swap_f.start()
    sent_all(snd, ms_sem, 64)
    sent_all(snd2, bs_sem, 64)
    sent_all(dtok, ts_sem, 8)
    sent_all(dps, cs_sem, 8)
    for cp in step1 + step2:
        cp.wait_send()
    for d in range(8):
        forward(d).wait_send()
    swap_f.wait()
    out[...] = (middle + (fin_s[...] + fin_r[...])).astype(BF)


def hand_over(a, b, c, a_out, b_out, c_out):
    a_out[...] = a[...]
    b_out[...] = b[...]
    c_out[...] = c[...]


def per_device(
    residual_in, lengths, cache_keys, cache_values, attend_gain, query_proj, key_proj,
    value_proj, lambdas, head_gain, out_proj, channel_gain, routes, route_weight,
    expert_gate, expert_up, expert_down, dense_gate, dense_up, dense_down, dense_mixer,
):
    inverse = np.float32(10000.0) ** (-np.arange(32, dtype=np.float32) / np.float32(32))
    frequency = jnp.asarray(np.tile(inverse, 4)[None, :])
    vm = pl.BlockSpec(memory_space=pltpu.VMEM)
    sm = pl.BlockSpec(memory_space=pltpu.SMEM)
    hb = pl.BlockSpec(memory_space=pl.ANY)
    DMA = pltpu.SemaphoreType.DMA
    V = pltpu.VMEM
    out, keys, values = pl.pallas_call(
        body,
        name="layer",
        out_shape=(
            jax.ShapeDtypeStruct((SEQS, WIDTH), BF),
            jax.ShapeDtypeStruct((SEQS, 128), BF),
            jax.ShapeDtypeStruct((SEQS, 128), BF),
        ),
        in_specs=[vm] * 6 + [sm] * 2 + [vm] * 2 + [hb] * 12,
        out_specs=(vm, vm, vm),
        scratch_shapes=[
            V((SEQS, LENGTH, 128), BF), V((SEQS, LENGTH, 128), BF),
            V((1024, 256), BF), V((1024, 128), BF), V((1024, 128), BF), V((256, 1024), BF),
            V((2, 1024, 256), BF), V((2, 1024, 256), BF), V((2, 256, 1024), BF),
            V((8, 2, 3, 16, 1024), BF),
            V((64, 128), F32), V((SEQS, 128), F32), V((SEQS, 128), F32),
            V((64, 128), F32),
            V((SEQS, WIDTH), BF), V((SEQS, WIDTH), BF), V((SEQS, WIDTH), BF),
            V((1024, 128), F32),
            V((64, 16, 128), BF), V((64, 16, 128), BF), V((64, 16, 128), BF), V((64, 16, 128), BF),
            V((8, 16, WIDTH), BF), V((8, 16, WIDTH), BF), V((8, 16, WIDTH), BF),
            V((SEQS, WIDTH), F32), V((SEQS, WIDTH), F32),
            DMA((7,)), DMA((16,)), DMA((16,)), DMA((3,)),
            DMA((8,)), DMA((8,)), DMA((8,)), DMA((8,)), DMA((3,)), DMA((3,)),
            DMA, DMA, DMA, DMA((8,)), DMA, DMA, DMA, DMA((8,)), DMA, DMA,
            DMA, DMA, pltpu.SemaphoreType.REGULAR,
        ],
        compiler_params=pltpu.CompilerParams(
            collective_id=0, has_side_effects=True, vmem_limit_bytes=60 * 1024 * 1024
        ),
    )(
        residual_in, attend_gain, channel_gain, dense_mixer, head_gain, frequency,
        lengths, lambdas, routes.T, route_weight.T,
        cache_keys.reshape(SEQS, LENGTH, 128), cache_values.reshape(SEQS, LENGTH, 128),
        query_proj, key_proj, value_proj, out_proj,
        expert_gate[0], expert_up[0], expert_down[0], dense_gate.T, dense_up.T, dense_down,
    )
    out, keys, values = pl.pallas_call(
        hand_over,
        name="hand_over",
        out_shape=(
            jax.ShapeDtypeStruct((SEQS, WIDTH), BF),
            jax.ShapeDtypeStruct((SEQS, 128), BF),
            jax.ShapeDtypeStruct((SEQS, 128), BF),
        ),
        in_specs=[vm] * 3,
        out_specs=(vm, vm, vm),
    )(out, keys, values)
    return out, keys.reshape(SEQS, 1, 128), values.reshape(SEQS, 1, 128)


def solution(mesh):
    placed = (
        P("ep", None), P("ep"), P("ep", "tp", None, None), P("ep", "tp", None, None), P(),
        P(None, "tp"), P(None, "tp"), P(None, "tp"), P("tp"), P(), P("tp", None), P(),
        P("ep", None), P("ep", None), P("ep", None, "tp"), P("ep", None, "tp"),
        P("ep", "tp", None), P(None, ("ep", "tp")), P(None, ("ep", "tp")),
        P(("ep", "tp"), None), P(),
    )
    return jax.shard_map(
        per_device, mesh=mesh, in_specs=placed,
        out_specs=(P("ep", None), P("ep", "tp", None), P("ep", "tp", None)),
        check_vma=False,
    )
```

```python
import jax
import jax.numpy as jnp
import numpy as np
from jax import lax
from jax.experimental import pallas as pl
from jax.experimental.pallas import tpu as pltpu
from jax.sharding import PartitionSpec as P

MESH = pl.DeviceIdType.MESH
BF = jnp.bfloat16
F32 = jnp.float32
EPS = 1e-06
NZ, NY, NX = 8, 4, 4
SEQS, WIDTH, LENGTH = 16, 1024, 1024


def norm(rows, gain):
    scale = lax.rsqrt(jnp.mean(rows * rows, axis=-1, keepdims=True) + EPS)
    return rows * scale * gain


def silu(v):
    return v / (1.0 + jnp.exp(-v))


def body(
    residual_h, attend_gain_h, channel_gain_h, mixer_h, head_gain_h, frequency_h,
    lengths_h, lambdas_h, routes_h, weights_h,
    cache_keys, cache_values, w_query, w_key, w_value, w_out,
    e_gate, e_up, e_down, d_gate, d_up, d_down,
    out_h, new_keys_h, new_values_h,
    residual, attend_gain, channel_gain, mixer, head_gain, frequency,
    lengths, lambdas, routes_turned, weight_turned, out, new_keys, new_values, in_sem, out_sem,
    kbuf, vbuf, wq, wk, wv, wo, egb, eub, edb, dwb,
    qs, kn, nv, att, pa, pb, nsb, sc, snd, rcv, snd2, rcv2, dtok, dps, dpr, fin_s, fin_r,
    load_sem, k_sem, v_sem, own_sem, zs_sem, zr_sem, ps_sem, pr_sem, es_sem, er_sem,
    xs_sem, xr_sem, ms_sem, mr_sem, ts_sem, tr_sem, bs_sem, br_sem, cs_sem, cr_sem,
    fs_sem, fr_sem, line_sem,
):
    ep = lax.axis_index("ep")
    c = lax.axis_index("tp")
    z = ep // 16
    y = (ep // 4) % 4
    x = ep % 4
    other = (ep, 1 - c)
    selfish = c == 0

    def chip(dz, dy, dx):
        return ((z + dz + NZ) % NZ) * 16 + ((y + dy) % 4) * 4 + (x + dx) % 4

    partners = []
    for p, dz in ((0, 0), (1, -1), (2, 1)):
        for dy in (2, 1, 3, 0):
            for dx in (2, 1, 3, 0):
                back = ((3 - p) % 3) * 16 + ((4 - dy) % 4) * 4 + (4 - dx) % 4
                partners.append((chip(4 * c + dz, dy, dx), p * 16 + dy * 4 + dx, back))
    for h in range(2):
        for dy in (2, 1, 3, 0):
            for j in range(2):
                back = 48 + (1 - h) * 8 + ((4 - dy) % 4) * 2 + (c + j) % 2
                partners.append((chip(2 + 4 * h, dy, c + 2 * j), 48 + h * 8 + dy * 2 + j, back))
    plane = []
    for dy in (2, 1, 3, 0):
        for j in range(2):
            plane.append((chip(0, dy, c + 2 * j), dy * 2 + j, ((4 - dy) % 4) * 2 + (c + j) % 2))

    def z_peer(d):
        return (((z + d) % NZ) * 16 + y * 4 + x, c)

    loads = [
        pltpu.make_async_copy(src, dst, load_sem.at[i])
        for i, (src, dst) in enumerate(
            [(w_query, wq), (w_key, wk), (w_value, wv), (w_out, wo),
             (e_gate, egb.at[c]), (e_up, eub.at[c]), (e_down, edb.at[c])]
        )
    ]
    own_parts = [
        pltpu.make_async_copy(src, dwb.at[z, c, i], own_sem.at[i])
        for i, src in enumerate([d_gate, d_up, d_down])
    ]
    kv = []
    for quarter in range(4):
        part = pl.ds(4 * quarter, 4)
        kv.append(
            (
                pltpu.make_async_copy(cache_keys.at[part], kbuf.at[part], k_sem.at[quarter]),
                pltpu.make_async_copy(cache_values.at[part], vbuf.at[part], v_sem.at[quarter]),
            )
        )
    small = [
        pltpu.make_async_copy(src, dst, in_sem.at[i])
        for i, (src, dst) in enumerate(
            [(residual_h, residual), (attend_gain_h, attend_gain), (frequency_h, frequency),
             (lengths_h, lengths), (lambdas_h, lambdas), (routes_h, routes_turned),
             (weights_h, weight_turned), (channel_gain_h, channel_gain), (mixer_h, mixer),
             (head_gain_h, head_gain)]
        )
    ]
    for cp in own_parts + small[:5]:
        cp.start()
    for i in range(3):
        loads[i].start()

    kv[0][0].start()
    kv[0][1].start()
    for kind in range(2):
        for quarter in (1, 2, 3):
            kv[quarter][kind].start()
    barrier = pltpu.get_barrier_semaphore()
    for d in (4, 3, 5, 2, 6, 1, 7):
        pl.semaphore_signal(barrier, inc=1, device_id=z_peer(d), device_id_type=MESH)
    for k in range(15, 0, -1):
        pl.semaphore_signal(
            barrier, inc=1, device_id=(chip(0, k // 4, k % 4), c), device_id_type=MESH
        )
    pl.semaphore_signal(barrier, inc=1, device_id=other, device_id_type=MESH)

    for cp in small[5:]:
        cp.start()
    loads[3].start()

    for cp in small[:5]:
        cp.wait()
    res = residual[...].astype(F32)
    normed = norm(res, attend_gain[...].astype(F32).reshape(1, WIDTH)).astype(BF)
    for i in range(3):
        loads[i].wait()
    q = jnp.dot(normed, wq[...], preferred_element_type=F32)
    kk = jnp.dot(normed, wk[...], preferred_element_type=F32)
    vv = jnp.dot(normed, wv[...], preferred_element_type=F32).astype(BF)
    lane128 = lax.broadcasted_iota(jnp.int32, (SEQS, 128), 1)
    row16 = lax.broadcasted_iota(jnp.int32, (SEQS, 128), 0)
    first = (lane128 % 64) < 32
    place = jnp.zeros((SEQS, 128), jnp.int32)
    for s in range(SEQS):
        place = jnp.where(row16 == s, lengths[s], place)
    angles = place.astype(F32) * frequency[...]
    cos_t, sin_t = jnp.cos(angles), jnp.sin(angles)
    sin_t = jnp.where(first, -sin_t, sin_t)

    def rotated(u):
        swapped = jnp.where(first, pltpu.roll(u, 96, 1), pltpu.roll(u, 32, 1))
        return (u * cos_t + swapped * sin_t).astype(BF)

    k_rot = rotated(kk)
    new_keys[...] = k_rot
    new_values[...] = vv
    results = [
        pltpu.make_async_copy(new_keys, new_keys_h, out_sem.at[0]),
        pltpu.make_async_copy(new_values, new_values_h, out_sem.at[1]),
    ]
    for cp in results:
        cp.start()
    kn[...] = k_rot.astype(F32)
    nv[...] = vv.astype(F32)
    for g in range(2):
        q_rot = rotated(q[:, 128 * g : 128 * g + 128]).astype(F32) * 0.125
        qs[pl.ds(g, SEQS, stride=4), :] = jnp.where(lane128 < 64, q_rot, 0.0)
        qs[pl.ds(2 + g, SEQS, stride=4), :] = jnp.where(lane128 < 64, 0.0, q_rot)

    pl.semaphore_wait(barrier, 7 + 15 + 1)
    for d in (4, 3, 5, 2, 6, 1, 7):
        pl.semaphore_signal(line_sem, inc=1, device_id=z_peer(d), device_id_type=MESH)

    def z_copy(d, hop):
        ref = dwb.at[(z + hop + d) % NZ, c]
        return pltpu.make_async_remote_copy(
            src_ref=ref, dst_ref=ref, send_sem=zs_sem.at[d], recv_sem=zr_sem.at[d],
            device_id=z_peer(hop), device_id_type=MESH,
        )

    def z_wait(d):
        ref = dwb.at[(z + d) % NZ, c]
        pltpu.make_async_copy(ref, ref, zr_sem.at[d % NZ]).wait()

    def forward(d):
        ref = dwb.at[(z + d) % NZ, c]
        return pltpu.make_async_remote_copy(
            src_ref=ref, dst_ref=ref, send_sem=ps_sem.at[d], recv_sem=pr_sem.at[d],
            device_id=other, device_id_type=MESH,
        )

    for cp in own_parts:
        cp.wait()
    step1 = [z_copy(4, 4), z_copy(7, 1), z_copy(1, -1)]
    for cp in step1:
        cp.start()
    swaps = [
        pltpu.make_async_remote_copy(
            src_ref=src, dst_ref=dst.at[c], send_sem=es_sem.at[i], recv_sem=er_sem.at[i],
            device_id=other, device_id_type=MESH,
        )
        for i, (src, dst) in enumerate([(e_gate, egb), (e_up, eub), (e_down, edb)])
    ]
    forward(0).start()

    sub8 = lax.broadcasted_iota(jnp.int32, (8, 1), 0)
    low8 = sub8 < 4
    lam = jnp.where(sub8 % 2 == 0, lambdas[0], lambdas[1])
    position = lax.broadcasted_iota(jnp.int32, (8, LENGTH), 1)
    turned = (((1,), (1,)), ((), ()))

    def attend(pairs):
        for quarter in sorted({p // 2 for p in pairs}):
            kv[quarter][0].wait()
        scores, own = [], []
        for p in pairs:
            query = qs[8 * p : 8 * p + 8, :]
            first_q = jnp.where(low8, query, 0.0).astype(BF)
            second_q = jnp.where(low8, 0.0, query).astype(BF)
            scores.append(
                lax.dot_general(first_q, kbuf[2 * p], turned, preferred_element_type=F32)
                + lax.dot_general(second_q, kbuf[2 * p + 1], turned, preferred_element_type=F32)
            )
            key = jnp.where(low8, kn[2 * p : 2 * p + 1, :], kn[2 * p + 1 : 2 * p + 2, :])
            own.append(
                jnp.exp(jnp.broadcast_to(jnp.sum(query * key, axis=-1, keepdims=True), (8, 128)))
            )
        weights, own_weights = [], []
        for i, p in enumerate(pairs):
            limit = jnp.where(low8, lengths[2 * p], lengths[2 * p + 1])
            e = jnp.where(position < limit, jnp.exp(scores[i]), 0.0)
            inverse = 1.0 / (jnp.sum(e, axis=-1, keepdims=True) + own[i])
            share = e * inverse[:, 0:1]
            share_own = own[i] * inverse
            weights.append((share - lam * pltpu.roll(share, 6, 0)).astype(BF))
            own_weights.append(
                (share_own - lam * pltpu.roll(share_own, 6, 0)).astype(BF).astype(F32)
            )
        for quarter in sorted({p // 2 for p in pairs}):
            kv[quarter][1].wait()
        for i, p in enumerate(pairs):
            first_a = jnp.dot(weights[i], vbuf[2 * p], preferred_element_type=F32)
            second_a = jnp.dot(weights[i], vbuf[2 * p + 1], preferred_element_type=F32)
            value = jnp.where(low8, nv[2 * p : 2 * p + 1, :], nv[2 * p + 1 : 2 * p + 2, :])
            att[8 * p : 8 * p + 8, :] = (
                jnp.where(low8, first_a, second_a) + own_weights[i] * value
            )

    attend((0, 1))

    attend((2, 3, 4, 5, 6, 7))

    for i in range(4, 7):
        loads[i].start()

    for cp in small[5:]:
        cp.wait()
    gain_h = head_gain[...].astype(F32).reshape(1, 128)
    rows = jnp.concatenate(
        [(norm(att[pl.ds(g, SEQS, stride=4), :], gain_h) * 0.8).astype(BF) for g in range(2)], axis=1
    )
    loads[3].wait()
    pa[...] = jnp.dot(rows, wo[...], preferred_element_type=F32).astype(BF)
    swap_a = pltpu.make_async_remote_copy(
        src_ref=pa, dst_ref=pb, send_sem=xs_sem, recv_sem=xr_sem,
        device_id=other, device_id_type=MESH,
    )
    swap_a.start()
    for cp in swaps:
        cp.start()

    row128 = lax.broadcasted_iota(jnp.int32, (128, SEQS), 0)
    block = row128 // 2
    in_half = block >= 48
    third = block // 16
    dz_t = jnp.where(in_half, 2 + 4 * ((block // 8) % 2), 4 * c + jnp.where(third == 2, 1, -third))
    dy_t = jnp.where(in_half, (block // 2) % 4, (block // 4) % 4)
    dx_t = jnp.where(in_half, c + 2 * (block % 2), block % 4)
    expert_t = ((z + dz_t + NZ) % NZ) * 16 + ((y + dy_t) % 4) * 4 + (x + dx_t) % 4
    hit_t = jnp.zeros((128, SEQS), F32)
    weight_t = jnp.zeros((128, SEQS), F32)
    for k in range(6):
        same = routes_turned[k : k + 1, :] == expert_t
        hit_t = hit_t + jnp.where(same, 1.0, 0.0)
        weight_t = weight_t + jnp.where(same, weight_turned[k : k + 1, :], 0.0)
    up_tri = jnp.where(
        lax.broadcasted_iota(jnp.int32, (SEQS, SEQS), 0)
        < lax.broadcasted_iota(jnp.int32, (SEQS, SEQS), 1),
        1.0, 0.0,
    )
    rank_t = jnp.dot(hit_t.astype(BF), up_tri.astype(BF), preferred_element_type=F32)
    pick_t = jnp.where(rank_t == (row128 % 2).astype(F32), hit_t, 0.0).astype(BF)

    combine_t = jnp.where(rank_t == (row128 % 2).astype(F32), weight_t, 0.0)
    c_hi = combine_t.astype(BF)
    rest = combine_t - c_hi.astype(F32)
    c_mid = rest.astype(BF)
    c_lo = (rest - c_mid.astype(F32)).astype(BF)
    eye = jnp.where(
        lax.broadcasted_iota(jnp.int32, (SEQS, SEQS), 0)
        == lax.broadcasted_iota(jnp.int32, (SEQS, SEQS), 1),
        1.0, 0.0,
    ).astype(BF)
    combine3 = jnp.concatenate(
        [
            lax.dot_general(eye, part, (((1,), (1,)), ((), ())), preferred_element_type=F32)
            for part in (c_hi, c_mid, c_lo)
        ],
        axis=0,
    ).astype(BF)

    swap_a.wait()
    middle = (res + (pa[...].astype(F32) + pb[...].astype(F32))).astype(BF).astype(F32)
    ns = norm(middle, channel_gain[...].astype(F32).reshape(1, WIDTH)).astype(BF)
    nsb[...] = ns
    switch = jax.nn.sigmoid(
        jnp.sum(ns.astype(F32) * mixer[...].astype(F32).reshape(1, WIDTH), axis=-1, keepdims=True)
    )

    def spread(values):
        for j in range(8):
            sc[pl.ds(j, 128, stride=8), :] = values[:, 128 * j : 128 * j + 128]

    def send_each(peers, pick_src, dst, send_sem, recv_sem):
        for target, here, there in peers:
            remote = pltpu.make_async_remote_copy(
                src_ref=pick_src(here), dst_ref=dst.at[there], send_sem=send_sem,
                recv_sem=recv_sem, device_id=(target, c), device_id_type=MESH,
            )
            if here:
                remote.start()
                continue

            @pl.when(selfish)
            def _():
                pltpu.make_async_copy(pick_src(0), dst.at[0], recv_sem).start()

            @pl.when(jnp.logical_not(selfish))
            def _(remote=remote):
                remote.start()

    def sent_all(buf, send_sem, count):
        @pl.when(selfish)
        def _():
            part = buf.at[pl.ds(0, count - 1)]
            pltpu.make_async_copy(part, part, send_sem).wait()

        @pl.when(jnp.logical_not(selfish))
        def _():
            pltpu.make_async_copy(buf, buf, send_sem).wait()

    picked = jnp.dot(pick_t, ns, preferred_element_type=F32)
    for j in range(8):
        sc[pl.ds(j, 128, stride=8), :] = picked[:, 128 * j : 128 * j + 128]
    snd[...] = sc[...].reshape(64, 16, 128).astype(BF)
    pl.semaphore_wait(line_sem, 7)
    send_each(partners, lambda n: snd.at[n], rcv, ms_sem, mr_sem)
    send_each(plane, lambda n: nsb, dtok, ts_sem, tr_sem)

    for d in (7, 1, 4):
        z_wait(d)
    step2 = [z_copy(6, 1), z_copy(2, -1), z_copy(3, 1), z_copy(5, -1)]
    for cp in step2:
        cp.start()
    for d in (1, 7, 4):
        forward(d).start()

    for i in range(4, 7):
        loads[i].wait()
    for cp in swaps:
        cp.wait()

    pltpu.make_async_copy(rcv, rcv, mr_sem).wait()
    sc[...] = rcv[...].reshape(1024, 128).astype(F32)
    rows = jnp.concatenate(
        [sc[pl.ds(j, 128, stride=8), :].astype(BF) for j in range(8)], axis=1
    )
    total = None
    for h in range(2):
        gate = jnp.dot(rows, egb[h], preferred_element_type=F32)
        upper = jnp.dot(rows, eub[h], preferred_element_type=F32)
        hidden = (silu(gate) * upper).astype(BF)
        half = jnp.dot(hidden, edb[h], preferred_element_type=F32).astype(BF).astype(F32)
        total = half if total is None else total + half
    for j in range(8):
        sc[pl.ds(j, 128, stride=8), :] = total[:, 128 * j : 128 * j + 128]
    snd2[...] = sc[...].reshape(64, 16, 128).astype(BF)
    send_each(partners, lambda n: snd2.at[n], rcv2, bs_sem, br_sem)

    for d in (2, 6, 3, 5):
        z_wait(d)
        forward(d).start()
    pltpu.make_async_copy(dtok, dtok, tr_sem).wait()
    for d in range(8):
        mirror = dwb.at[(z + d) % NZ, 1 - c]
        pltpu.make_async_copy(mirror, mirror, pr_sem.at[d]).wait()
    xd = dtok[...].reshape(128, WIDTH)
    gate_w = dwb[:, :, 0].reshape(256, WIDTH)
    up_w = dwb[:, :, 1].reshape(256, WIDTH)
    down_w = dwb[:, :, 2].reshape(256, WIDTH)
    gate = lax.dot_general(xd, gate_w, turned, preferred_element_type=F32)
    upper = lax.dot_general(xd, up_w, turned, preferred_element_type=F32)
    hidden = (silu(gate) * upper).astype(BF)
    dps[...] = jnp.dot(hidden, down_w, preferred_element_type=F32).astype(BF).reshape(8, 16, WIDTH)
    send_each(plane, lambda n: dps.at[n], dpr, cs_sem, cr_sem)

    pltpu.make_async_copy(rcv2, rcv2, br_sem).wait()
    sc[...] = rcv2[...].reshape(1024, 128).astype(F32)
    returned = jnp.concatenate(
        [sc[pl.ds(j, 128, stride=8), :].astype(BF) for j in range(8)], axis=1
    )
    three = jnp.dot(combine3, returned, preferred_element_type=F32)
    routed = three[0:16] + (three[16:32] + three[32:48])
    pltpu.make_async_copy(dpr, dpr, cr_sem).wait()
    dense = dpr[0].astype(F32)
    for i in range(1, 8):
        dense = dense + dpr[i].astype(F32)
    fin_s[...] = routed + switch * dense
    swap_f = pltpu.make_async_remote_copy(
        src_ref=fin_s, dst_ref=fin_r, send_sem=fs_sem, recv_sem=fr_sem,
        device_id=other, device_id_type=MESH,
    )
    swap_f.start()
    sent_all(snd, ms_sem, 64)
    sent_all(snd2, bs_sem, 64)
    sent_all(dtok, ts_sem, 8)
    sent_all(dps, cs_sem, 8)
    for cp in step1 + step2:
        cp.wait_send()
    for d in range(8):
        forward(d).wait_send()
    swap_f.wait()
    out[...] = (middle + (fin_s[...] + fin_r[...])).astype(BF)
    last = pltpu.make_async_copy(out, out_h, out_sem.at[2])
    last.start()
    for cp in results + [last]:
        cp.wait()


def hand_over(a, b, c, a_out, b_out, c_out):
    a_out[...] = a[...]
    b_out[...] = b[...]
    c_out[...] = c[...]


def per_device(
    residual_in, lengths, cache_keys, cache_values, attend_gain, query_proj, key_proj,
    value_proj, lambdas, head_gain, out_proj, channel_gain, routes, route_weight,
    expert_gate, expert_up, expert_down, dense_gate, dense_up, dense_down, dense_mixer,
):
    inverse = np.float32(10000.0) ** (-np.arange(32, dtype=np.float32) / np.float32(32))
    frequency = jnp.asarray(np.tile(inverse, 4)[None, :])
    vm = pl.BlockSpec(memory_space=pltpu.VMEM)
    hb = pl.BlockSpec(memory_space=pl.ANY)
    DMA = pltpu.SemaphoreType.DMA
    V = pltpu.VMEM
    out, keys, values = pl.pallas_call(
        body,
        name="layer",
        out_shape=(
            jax.ShapeDtypeStruct((SEQS, WIDTH), BF),
            jax.ShapeDtypeStruct((SEQS, 128), BF),
            jax.ShapeDtypeStruct((SEQS, 128), BF),
        ),
        in_specs=[hb] * 22,
        out_specs=(hb, hb, hb),
        scratch_shapes=[
            V((SEQS, WIDTH), BF), V((WIDTH,), BF), V((WIDTH,), BF), V((WIDTH,), BF),
            V((128,), BF), V((1, 128), F32), pltpu.SMEM((SEQS,), jnp.int32),
            pltpu.SMEM((2,), F32), V((6, SEQS), jnp.int32), V((6, SEQS), F32),
            V((SEQS, WIDTH), BF), V((SEQS, 128), BF), V((SEQS, 128), BF), DMA((10,)), DMA((3,)),
            V((SEQS, LENGTH, 128), BF), V((SEQS, LENGTH, 128), BF),
            V((1024, 256), BF), V((1024, 128), BF), V((1024, 128), BF), V((256, 1024), BF),
            V((2, 1024, 256), BF), V((2, 1024, 256), BF), V((2, 256, 1024), BF),
            V((8, 2, 3, 16, 1024), BF),
            V((64, 128), F32), V((SEQS, 128), F32), V((SEQS, 128), F32),
            V((64, 128), F32),
            V((SEQS, WIDTH), BF), V((SEQS, WIDTH), BF), V((SEQS, WIDTH), BF),
            V((1024, 128), F32),
            V((64, 16, 128), BF), V((64, 16, 128), BF), V((64, 16, 128), BF), V((64, 16, 128), BF),
            V((8, 16, WIDTH), BF), V((8, 16, WIDTH), BF), V((8, 16, WIDTH), BF),
            V((SEQS, WIDTH), F32), V((SEQS, WIDTH), F32),
            DMA((7,)), DMA((4,)), DMA((4,)), DMA((3,)),
            DMA((8,)), DMA((8,)), DMA((8,)), DMA((8,)), DMA((3,)), DMA((3,)),
            DMA, DMA, DMA, DMA, DMA, DMA, DMA, DMA, DMA, DMA,
            DMA, DMA, pltpu.SemaphoreType.REGULAR,
        ],
        compiler_params=pltpu.CompilerParams(
            collective_id=0, has_side_effects=True, vmem_limit_bytes=60 * 1024 * 1024
        ),
    )(
        residual_in, attend_gain, channel_gain, dense_mixer, head_gain, frequency,
        lengths, lambdas, routes.T, route_weight.T,
        cache_keys.reshape(SEQS, LENGTH, 128), cache_values.reshape(SEQS, LENGTH, 128),
        query_proj, key_proj, value_proj, out_proj,
        expert_gate[0], expert_up[0], expert_down[0], dense_gate.T, dense_up.T, dense_down,
    )
    out, keys, values = pl.pallas_call(
        hand_over,
        name="hand_over",
        out_shape=(
            jax.ShapeDtypeStruct((SEQS, WIDTH), BF),
            jax.ShapeDtypeStruct((SEQS, 128), BF),
            jax.ShapeDtypeStruct((SEQS, 128), BF),
        ),
        in_specs=[vm] * 3,
        out_specs=(vm, vm, vm),
    )(out, keys, values)
    return out, keys.reshape(SEQS, 1, 128), values.reshape(SEQS, 1, 128)


def solution(mesh):
    placed = (
        P("ep", None), P("ep"), P("ep", "tp", None, None), P("ep", "tp", None, None), P(),
        P(None, "tp"), P(None, "tp"), P(None, "tp"), P("tp"), P(), P("tp", None), P(),
        P("ep", None), P("ep", None), P("ep", None, "tp"), P("ep", None, "tp"),
        P("ep", "tp", None), P(None, ("ep", "tp")), P(None, ("ep", "tp")),
        P(("ep", "tp"), None), P(),
    )
    return jax.shard_map(
        per_device, mesh=mesh, in_specs=placed,
        out_specs=(P("ep", None), P("ep", "tp", None), P("ep", "tp", None)),
        check_vma=False,
    )
```

```python
import jax
import jax.numpy as jnp
import numpy as np
from jax import lax
from jax.experimental import pallas as pl
from jax.experimental.pallas import tpu as pltpu
from jax.sharding import PartitionSpec as P

MESH = pl.DeviceIdType.MESH
BF = jnp.bfloat16
F32 = jnp.float32
EPS = 1e-06
NZ, NY, NX = 8, 4, 4
SEQS, WIDTH, LENGTH = 16, 1024, 1024


def norm(rows, gain):
    scale = lax.rsqrt(jnp.mean(rows * rows, axis=-1, keepdims=True) + EPS)
    return rows * scale * gain


def silu(v):
    return v / (1.0 + jnp.exp(-v))


def body(
    residual_h, attend_gain_h, channel_gain_h, mixer_h, head_gain_h, frequency_h,
    lengths_h, lambdas_h, routes_h, weights_h,
    cache_keys, cache_values, w_query, w_key, w_value, w_out,
    e_gate, e_up, e_down, d_gate, d_up, d_down,
    out_h, new_keys_h, new_values_h,
    residual, attend_gain, channel_gain, mixer, head_gain, frequency,
    lengths, lambdas, routes_turned, weight_turned, out, new_keys, new_values, in_sem, out_sem,
    kbuf, vbuf, wq, wk, wv, wo, egb, eub, edb, dwb,
    qs, kn, nv, att, pa, pb, nsb, sc, snd, rcv, snd2, rcv2, dtok, dps, dpr, fin_s, fin_r,
    load_sem, k_sem, v_sem, own_sem, zs_sem, zr_sem, ps_sem, pr_sem, es_sem, er_sem,
    xs_sem, xr_sem, ms_sem, mr_sem, ts_sem, tr_sem, bs_sem, br_sem, cs_sem, cr_sem,
    fs_sem, fr_sem, line_sem,
):
    ep = lax.axis_index("ep")
    c = lax.axis_index("tp")
    z = ep // 16
    y = (ep // 4) % 4
    x = ep % 4
    other = (ep, 1 - c)
    selfish = c == 0

    def chip(dz, dy, dx):
        return ((z + dz + NZ) % NZ) * 16 + ((y + dy) % 4) * 4 + (x + dx) % 4

    partners = []
    for p, dz in ((0, 0), (1, -1), (2, 1)):
        for dy in (2, 1, 3, 0):
            for dx in (2, 1, 3, 0):
                back = ((3 - p) % 3) * 16 + ((4 - dy) % 4) * 4 + (4 - dx) % 4
                partners.append((chip(4 * c + dz, dy, dx), p * 16 + dy * 4 + dx, back))
    for h in range(2):
        for dy in (2, 1, 3, 0):
            for j in range(2):
                back = 48 + (1 - h) * 8 + ((4 - dy) % 4) * 2 + (c + j) % 2
                partners.append((chip(2 + 4 * h, dy, c + 2 * j), 48 + h * 8 + dy * 2 + j, back))
    plane = []
    for dy in (2, 1, 3, 0):
        for j in range(2):
            plane.append((chip(0, dy, c + 2 * j), dy * 2 + j, ((4 - dy) % 4) * 2 + (c + j) % 2))

    def z_peer(d):
        return (((z + d) % NZ) * 16 + y * 4 + x, c)

    loads = [
        pltpu.make_async_copy(src, dst, load_sem.at[i])
        for i, (src, dst) in enumerate(
            [(w_query, wq), (w_key, wk), (w_value, wv), (w_out, wo),
             (e_gate, egb.at[c]), (e_up, eub.at[c]), (e_down, edb.at[c])]
        )
    ]
    own_parts = [
        pltpu.make_async_copy(src, dwb.at[z, c, i], own_sem.at[i])
        for i, src in enumerate([d_gate, d_up, d_down])
    ]
    kv = []
    for quarter in range(4):
        part = pl.ds(4 * quarter, 4)
        kv.append(
            (
                pltpu.make_async_copy(cache_keys.at[part], kbuf.at[part], k_sem.at[quarter]),
                pltpu.make_async_copy(cache_values.at[part], vbuf.at[part], v_sem.at[quarter]),
            )
        )
    small = [
        pltpu.make_async_copy(src, dst, in_sem.at[i])
        for i, (src, dst) in enumerate(
            [(residual_h, residual), (attend_gain_h, attend_gain), (frequency_h, frequency),
             (lengths_h, lengths), (lambdas_h, lambdas), (routes_h, routes_turned),
             (weights_h, weight_turned), (channel_gain_h, channel_gain), (mixer_h, mixer),
             (head_gain_h, head_gain)]
        )
    ]
    for cp in own_parts + small[:5]:
        cp.start()
    for i in range(3):
        loads[i].start()

    barrier = pltpu.get_barrier_semaphore()
    for d in (4, 3, 5, 2, 6, 1, 7):
        pl.semaphore_signal(barrier, inc=1, device_id=z_peer(d), device_id_type=MESH)
    for k in range(15, 0, -1):
        pl.semaphore_signal(
            barrier, inc=1, device_id=(chip(0, k // 4, k % 4), c), device_id_type=MESH
        )
    pl.semaphore_signal(barrier, inc=1, device_id=other, device_id_type=MESH)

    for keys, values in kv:
        keys.start()
        values.start()
    for cp in small[5:]:
        cp.start()
    loads[3].start()

    for cp in small[:5]:
        cp.wait()
    res = residual[...].astype(F32)
    normed = norm(res, attend_gain[...].astype(F32).reshape(1, WIDTH)).astype(BF)
    for i in range(3):
        loads[i].wait()
    q = jnp.dot(normed, wq[...], preferred_element_type=F32)
    kk = jnp.dot(normed, wk[...], preferred_element_type=F32)
    vv = jnp.dot(normed, wv[...], preferred_element_type=F32).astype(BF)
    lane128 = lax.broadcasted_iota(jnp.int32, (SEQS, 128), 1)
    row16 = lax.broadcasted_iota(jnp.int32, (SEQS, 128), 0)
    first = (lane128 % 64) < 32
    place = jnp.zeros((SEQS, 128), jnp.int32)
    for s in range(SEQS):
        place = jnp.where(row16 == s, lengths[s], place)
    angles = place.astype(F32) * frequency[...]
    cos_t, sin_t = jnp.cos(angles), jnp.sin(angles)
    sin_t = jnp.where(first, -sin_t, sin_t)

    def rotated(u):
        swapped = jnp.where(first, pltpu.roll(u, 96, 1), pltpu.roll(u, 32, 1))
        return (u * cos_t + swapped * sin_t).astype(BF)

    k_rot = rotated(kk)
    new_keys[...] = k_rot
    new_values[...] = vv
    results = [
        pltpu.make_async_copy(new_keys, new_keys_h, out_sem.at[0]),
        pltpu.make_async_copy(new_values, new_values_h, out_sem.at[1]),
    ]
    for cp in results:
        cp.start()
    kn[...] = k_rot.astype(F32)
    nv[...] = vv.astype(F32)
    for g in range(2):
        q_rot = rotated(q[:, 128 * g : 128 * g + 128]).astype(F32) * 0.125
        qs[pl.ds(g, SEQS, stride=4), :] = jnp.where(lane128 < 64, q_rot, 0.0)
        qs[pl.ds(2 + g, SEQS, stride=4), :] = jnp.where(lane128 < 64, 0.0, q_rot)

    pl.semaphore_wait(barrier, 7 + 15 + 1)
    for d in (4, 3, 5, 2, 6, 1, 7):
        pl.semaphore_signal(line_sem, inc=1, device_id=z_peer(d), device_id_type=MESH)

    moved = []

    def z_send(d, hop, part):
        ref = dwb.at[(z + hop + d) % NZ, c, part]
        copy = pltpu.make_async_remote_copy(
            src_ref=ref, dst_ref=ref, send_sem=zs_sem.at[d, part], recv_sem=zr_sem.at[d, part],
            device_id=z_peer(hop), device_id_type=MESH,
        )
        copy.start()
        moved.append(copy)

    def z_wait(d, part):
        ref = dwb.at[(z + d) % NZ, c, part]
        pltpu.make_async_copy(ref, ref, zr_sem.at[d, part]).wait()

    def relay(part):
        z_wait(7, part)
        z_wait(1, part)
        z_send(6, 1, part)
        z_send(2, -1, part)

    def forward(d):
        ref = dwb.at[(z + d) % NZ, c]
        return pltpu.make_async_remote_copy(
            src_ref=ref, dst_ref=ref, send_sem=ps_sem.at[d], recv_sem=pr_sem.at[d],
            device_id=other, device_id_type=MESH,
        )

    for cp in own_parts:
        cp.wait()
    for part in range(3):
        z_send(7, 1, part)
        z_send(1, -1, part)
    z_send(6, 2, 0)
    z_send(2, -2, 0)
    swaps = [
        pltpu.make_async_remote_copy(
            src_ref=src, dst_ref=dst.at[c], send_sem=es_sem.at[i], recv_sem=er_sem.at[i],
            device_id=other, device_id_type=MESH,
        )
        for i, (src, dst) in enumerate([(e_gate, egb), (e_up, eub), (e_down, edb)])
    ]
    forward(0).start()

    sub8 = lax.broadcasted_iota(jnp.int32, (8, 1), 0)
    low8 = sub8 < 4
    lam = jnp.where(sub8 % 2 == 0, lambdas[0], lambdas[1])
    position = lax.broadcasted_iota(jnp.int32, (8, LENGTH), 1)
    turned = (((1,), (1,)), ((), ()))

    def attend(pairs):
        for quarter in sorted({p // 2 for p in pairs}):
            kv[quarter][0].wait()
        scores, own = [], []
        for p in pairs:
            query = qs[8 * p : 8 * p + 8, :]
            first_q = jnp.where(low8, query, 0.0).astype(BF)
            second_q = jnp.where(low8, 0.0, query).astype(BF)
            scores.append(
                lax.dot_general(first_q, kbuf[2 * p], turned, preferred_element_type=F32)
                + lax.dot_general(second_q, kbuf[2 * p + 1], turned, preferred_element_type=F32)
            )
            key = jnp.where(low8, kn[2 * p : 2 * p + 1, :], kn[2 * p + 1 : 2 * p + 2, :])
            own.append(
                jnp.exp(jnp.broadcast_to(jnp.sum(query * key, axis=-1, keepdims=True), (8, 128)))
            )
        weights, own_weights = [], []
        for i, p in enumerate(pairs):
            limit = jnp.where(low8, lengths[2 * p], lengths[2 * p + 1])
            e = jnp.where(position < limit, jnp.exp(scores[i]), 0.0)
            inverse = 1.0 / (jnp.sum(e, axis=-1, keepdims=True) + own[i])
            share = e * inverse[:, 0:1]
            share_own = own[i] * inverse
            weights.append((share - lam * pltpu.roll(share, 6, 0)).astype(BF))
            own_weights.append(
                (share_own - lam * pltpu.roll(share_own, 6, 0)).astype(BF).astype(F32)
            )
        for quarter in sorted({p // 2 for p in pairs}):
            kv[quarter][1].wait()
        for i, p in enumerate(pairs):
            first_a = jnp.dot(weights[i], vbuf[2 * p], preferred_element_type=F32)
            second_a = jnp.dot(weights[i], vbuf[2 * p + 1], preferred_element_type=F32)
            value = jnp.where(low8, nv[2 * p : 2 * p + 1, :], nv[2 * p + 1 : 2 * p + 2, :])
            att[8 * p : 8 * p + 8, :] = (
                jnp.where(low8, first_a, second_a) + own_weights[i] * value
            )

    attend((0, 1))

    attend((2, 3))
    attend((4, 5, 6, 7))

    for i in range(4, 7):
        loads[i].start()

    for cp in small[5:]:
        cp.wait()
    gain_h = head_gain[...].astype(F32).reshape(1, 128)
    rows = jnp.concatenate(
        [(norm(att[pl.ds(g, SEQS, stride=4), :], gain_h) * 0.8).astype(BF) for g in range(2)], axis=1
    )
    loads[3].wait()
    pa[...] = jnp.dot(rows, wo[...], preferred_element_type=F32).astype(BF)
    swap_a = pltpu.make_async_remote_copy(
        src_ref=pa, dst_ref=pb, send_sem=xs_sem, recv_sem=xr_sem,
        device_id=other, device_id_type=MESH,
    )
    swap_a.start()
    for cp in swaps:
        cp.start()

    relay(1)
    row128 = lax.broadcasted_iota(jnp.int32, (128, SEQS), 0)
    block = row128 // 2
    in_half = block >= 48
    third = block // 16
    dz_t = jnp.where(in_half, 2 + 4 * ((block // 8) % 2), 4 * c + jnp.where(third == 2, 1, -third))
    dy_t = jnp.where(in_half, (block // 2) % 4, (block // 4) % 4)
    dx_t = jnp.where(in_half, c + 2 * (block % 2), block % 4)
    expert_t = ((z + dz_t + NZ) % NZ) * 16 + ((y + dy_t) % 4) * 4 + (x + dx_t) % 4
    hit_t = jnp.zeros((128, SEQS), F32)
    weight_t = jnp.zeros((128, SEQS), F32)
    for k in range(6):
        same = routes_turned[k : k + 1, :] == expert_t
        hit_t = hit_t + jnp.where(same, 1.0, 0.0)
        weight_t = weight_t + jnp.where(same, weight_turned[k : k + 1, :], 0.0)
    up_tri = jnp.where(
        lax.broadcasted_iota(jnp.int32, (SEQS, SEQS), 0)
        < lax.broadcasted_iota(jnp.int32, (SEQS, SEQS), 1),
        1.0, 0.0,
    )
    rank_t = jnp.dot(hit_t.astype(BF), up_tri.astype(BF), preferred_element_type=F32)
    pick_t = jnp.where(rank_t == (row128 % 2).astype(F32), hit_t, 0.0).astype(BF)

    combine_t = jnp.where(rank_t == (row128 % 2).astype(F32), weight_t, 0.0)
    c_hi = combine_t.astype(BF)
    rest = combine_t - c_hi.astype(F32)
    c_mid = rest.astype(BF)
    c_lo = (rest - c_mid.astype(F32)).astype(BF)
    eye = jnp.where(
        lax.broadcasted_iota(jnp.int32, (SEQS, SEQS), 0)
        == lax.broadcasted_iota(jnp.int32, (SEQS, SEQS), 1),
        1.0, 0.0,
    ).astype(BF)
    combine3 = jnp.concatenate(
        [
            lax.dot_general(eye, part, (((1,), (1,)), ((), ())), preferred_element_type=F32)
            for part in (c_hi, c_mid, c_lo)
        ],
        axis=0,
    ).astype(BF)

    swap_a.wait()
    relay(2)
    middle = (res + (pa[...].astype(F32) + pb[...].astype(F32))).astype(BF).astype(F32)
    ns = norm(middle, channel_gain[...].astype(F32).reshape(1, WIDTH)).astype(BF)
    nsb[...] = ns
    switch = jax.nn.sigmoid(
        jnp.sum(ns.astype(F32) * mixer[...].astype(F32).reshape(1, WIDTH), axis=-1, keepdims=True)
    )

    def spread(values):
        for j in range(8):
            sc[pl.ds(j, 128, stride=8), :] = values[:, 128 * j : 128 * j + 128]

    def send_each(peers, pick_src, dst, send_sem, recv_sem):
        for target, here, there in peers:
            remote = pltpu.make_async_remote_copy(
                src_ref=pick_src(here), dst_ref=dst.at[there], send_sem=send_sem,
                recv_sem=recv_sem, device_id=(target, c), device_id_type=MESH,
            )
            if here:
                remote.start()
                continue

            @pl.when(selfish)
            def _():
                pltpu.make_async_copy(pick_src(0), dst.at[0], recv_sem).start()

            @pl.when(jnp.logical_not(selfish))
            def _(remote=remote):
                remote.start()

    def sent_all(buf, send_sem, count):
        @pl.when(selfish)
        def _():
            part = buf.at[pl.ds(0, count - 1)]
            pltpu.make_async_copy(part, part, send_sem).wait()

        @pl.when(jnp.logical_not(selfish))
        def _():
            pltpu.make_async_copy(buf, buf, send_sem).wait()

    picked = jnp.dot(pick_t, ns, preferred_element_type=F32)
    for j in range(8):
        sc[pl.ds(j, 128, stride=8), :] = picked[:, 128 * j : 128 * j + 128]
    snd[...] = sc[...].reshape(64, 16, 128).astype(BF)
    pl.semaphore_wait(line_sem, 7)
    send_each(partners, lambda n: snd.at[n], rcv, ms_sem, mr_sem)
    send_each(plane, lambda n: nsb, dtok, ts_sem, tr_sem)

    z_wait(7, 0)
    z_wait(1, 0)
    forward(7).start()
    forward(1).start()
    for part in range(3):
        z_wait(6, part)
        z_send(5, 1, part)
        z_wait(2, part)
        z_send(3, -1, part)
    for part in range(3):
        z_send(4, 2 - 4 * c, part)
    forward(6).start()
    forward(2).start()

    for i in range(4, 7):
        loads[i].wait()
    for cp in swaps:
        cp.wait()

    pltpu.make_async_copy(rcv, rcv, mr_sem).wait()
    sc[...] = rcv[...].reshape(1024, 128).astype(F32)
    rows = jnp.concatenate(
        [sc[pl.ds(j, 128, stride=8), :].astype(BF) for j in range(8)], axis=1
    )
    total = None
    for h in range(2):
        gate = jnp.dot(rows, egb[h], preferred_element_type=F32)
        upper = jnp.dot(rows, eub[h], preferred_element_type=F32)
        hidden = (silu(gate) * upper).astype(BF)
        half = jnp.dot(hidden, edb[h], preferred_element_type=F32).astype(BF).astype(F32)
        total = half if total is None else total + half
    for j in range(8):
        sc[pl.ds(j, 128, stride=8), :] = total[:, 128 * j : 128 * j + 128]
    snd2[...] = sc[...].reshape(64, 16, 128).astype(BF)
    send_each(partners, lambda n: snd2.at[n], rcv2, bs_sem, br_sem)

    for d in (3, 5, 4):
        for part in range(3):
            z_wait(d, part)
        forward(d).start()
    pltpu.make_async_copy(dtok, dtok, tr_sem).wait()
    for d in range(8):
        mirror = dwb.at[(z + d) % NZ, 1 - c]
        pltpu.make_async_copy(mirror, mirror, pr_sem.at[d]).wait()
    xd = dtok[...].reshape(128, WIDTH)
    gate_w = dwb[:, :, 0].reshape(256, WIDTH)
    up_w = dwb[:, :, 1].reshape(256, WIDTH)
    down_w = dwb[:, :, 2].reshape(256, WIDTH)
    gate = lax.dot_general(xd, gate_w, turned, preferred_element_type=F32)
    upper = lax.dot_general(xd, up_w, turned, preferred_element_type=F32)
    hidden = (silu(gate) * upper).astype(BF)
    dps[...] = jnp.dot(hidden, down_w, preferred_element_type=F32).astype(BF).reshape(8, 16, WIDTH)
    send_each(plane, lambda n: dps.at[n], dpr, cs_sem, cr_sem)

    pltpu.make_async_copy(rcv2, rcv2, br_sem).wait()
    sc[...] = rcv2[...].reshape(1024, 128).astype(F32)
    returned = jnp.concatenate(
        [sc[pl.ds(j, 128, stride=8), :].astype(BF) for j in range(8)], axis=1
    )
    three = jnp.dot(combine3, returned, preferred_element_type=F32)
    routed = three[0:16] + (three[16:32] + three[32:48])
    pltpu.make_async_copy(dpr, dpr, cr_sem).wait()
    dense = dpr[0].astype(F32)
    for i in range(1, 8):
        dense = dense + dpr[i].astype(F32)
    fin_s[...] = routed + switch * dense
    swap_f = pltpu.make_async_remote_copy(
        src_ref=fin_s, dst_ref=fin_r, send_sem=fs_sem, recv_sem=fr_sem,
        device_id=other, device_id_type=MESH,
    )
    swap_f.start()
    sent_all(snd, ms_sem, 64)
    sent_all(snd2, bs_sem, 64)
    sent_all(dtok, ts_sem, 8)
    sent_all(dps, cs_sem, 8)
    for cp in moved:
        cp.wait_send()
    for d in range(8):
        forward(d).wait_send()
    swap_f.wait()
    out[...] = (middle + (fin_s[...] + fin_r[...])).astype(BF)
    last = pltpu.make_async_copy(out, out_h, out_sem.at[2])
    last.start()
    for cp in results + [last]:
        cp.wait()


def hand_over(a, b, c, a_out, b_out, c_out):
    a_out[...] = a[...]
    b_out[...] = b[...]
    c_out[...] = c[...]


def per_device(
    residual_in, lengths, cache_keys, cache_values, attend_gain, query_proj, key_proj,
    value_proj, lambdas, head_gain, out_proj, channel_gain, routes, route_weight,
    expert_gate, expert_up, expert_down, dense_gate, dense_up, dense_down, dense_mixer,
):
    inverse = np.float32(10000.0) ** (-np.arange(32, dtype=np.float32) / np.float32(32))
    frequency = jnp.asarray(np.tile(inverse, 4)[None, :])
    vm = pl.BlockSpec(memory_space=pltpu.VMEM)
    hb = pl.BlockSpec(memory_space=pl.ANY)
    DMA = pltpu.SemaphoreType.DMA
    V = pltpu.VMEM
    out, keys, values = pl.pallas_call(
        body,
        name="layer",
        out_shape=(
            jax.ShapeDtypeStruct((SEQS, WIDTH), BF),
            jax.ShapeDtypeStruct((SEQS, 128), BF),
            jax.ShapeDtypeStruct((SEQS, 128), BF),
        ),
        in_specs=[hb] * 22,
        out_specs=(hb, hb, hb),
        scratch_shapes=[
            V((SEQS, WIDTH), BF), V((WIDTH,), BF), V((WIDTH,), BF), V((WIDTH,), BF),
            V((128,), BF), V((1, 128), F32), pltpu.SMEM((SEQS,), jnp.int32),
            pltpu.SMEM((2,), F32), V((6, SEQS), jnp.int32), V((6, SEQS), F32),
            V((SEQS, WIDTH), BF), V((SEQS, 128), BF), V((SEQS, 128), BF), DMA((10,)), DMA((3,)),
            V((SEQS, LENGTH, 128), BF), V((SEQS, LENGTH, 128), BF),
            V((1024, 256), BF), V((1024, 128), BF), V((1024, 128), BF), V((256, 1024), BF),
            V((2, 1024, 256), BF), V((2, 1024, 256), BF), V((2, 256, 1024), BF),
            V((8, 2, 3, 16, 1024), BF),
            V((64, 128), F32), V((SEQS, 128), F32), V((SEQS, 128), F32),
            V((64, 128), F32),
            V((SEQS, WIDTH), BF), V((SEQS, WIDTH), BF), V((SEQS, WIDTH), BF),
            V((1024, 128), F32),
            V((64, 16, 128), BF), V((64, 16, 128), BF), V((64, 16, 128), BF), V((64, 16, 128), BF),
            V((8, 16, WIDTH), BF), V((8, 16, WIDTH), BF), V((8, 16, WIDTH), BF),
            V((SEQS, WIDTH), F32), V((SEQS, WIDTH), F32),
            DMA((7,)), DMA((4,)), DMA((4,)), DMA((3,)),
            DMA((8, 3)), DMA((8, 3)), DMA((8,)), DMA((8,)), DMA((3,)), DMA((3,)),
            DMA, DMA, DMA, DMA, DMA, DMA, DMA, DMA, DMA, DMA,
            DMA, DMA, pltpu.SemaphoreType.REGULAR,
        ],
        compiler_params=pltpu.CompilerParams(
            collective_id=0, has_side_effects=True, vmem_limit_bytes=60 * 1024 * 1024
        ),
    )(
        residual_in, attend_gain, channel_gain, dense_mixer, head_gain, frequency,
        lengths, lambdas, routes.T, route_weight.T,
        cache_keys.reshape(SEQS, LENGTH, 128), cache_values.reshape(SEQS, LENGTH, 128),
        query_proj, key_proj, value_proj, out_proj,
        expert_gate[0], expert_up[0], expert_down[0], dense_gate.T, dense_up.T, dense_down,
    )
    out, keys, values = pl.pallas_call(
        hand_over,
        name="hand_over",
        out_shape=(
            jax.ShapeDtypeStruct((SEQS, WIDTH), BF),
            jax.ShapeDtypeStruct((SEQS, 128), BF),
            jax.ShapeDtypeStruct((SEQS, 128), BF),
        ),
        in_specs=[vm] * 3,
        out_specs=(vm, vm, vm),
    )(out, keys, values)
    return out, keys.reshape(SEQS, 1, 128), values.reshape(SEQS, 1, 128)


def solution(mesh):
    placed = (
        P("ep", None), P("ep"), P("ep", "tp", None, None), P("ep", "tp", None, None), P(),
        P(None, "tp"), P(None, "tp"), P(None, "tp"), P("tp"), P(), P("tp", None), P(),
        P("ep", None), P("ep", None), P("ep", None, "tp"), P("ep", None, "tp"),
        P("ep", "tp", None), P(None, ("ep", "tp")), P(None, ("ep", "tp")),
        P(("ep", "tp"), None), P(),
    )
    return jax.shard_map(
        per_device, mesh=mesh, in_specs=placed,
        out_specs=(P("ep", None), P("ep", "tp", None), P("ep", "tp", None)),
        check_vma=False,
    )
```

```python
import jax
import jax.numpy as jnp
import numpy as np
from jax import lax
from jax.experimental import pallas as pl
from jax.experimental.pallas import tpu as pltpu
from jax.sharding import PartitionSpec as P

MESH = pl.DeviceIdType.MESH
BF = jnp.bfloat16
F32 = jnp.float32
EPS = 1e-06
NZ, NY, NX = 8, 4, 4
SEQS, WIDTH, LENGTH = 16, 1024, 1024


def norm(rows, gain):
    scale = lax.rsqrt(jnp.mean(rows * rows, axis=-1, keepdims=True) + EPS)
    return rows * scale * gain


def silu(v):
    return v / (1.0 + jnp.exp(-v))


def body(
    residual_h, attend_gain_h, channel_gain_h, mixer_h, head_gain_h, frequency_h,
    lengths_h, lambdas_h, routes_h, weights_h,
    cache_keys, cache_values, w_query, w_key, w_value, w_out,
    e_gate, e_up, e_down, d_gate, d_up, d_down,
    out_h, new_keys_h, new_values_h,
    residual, attend_gain, channel_gain, mixer, head_gain, frequency,
    lengths, lambdas, routes_turned, weight_turned, out, new_keys, new_values, in_sem, out_sem,
    kbuf, vbuf, wq, wk, wv, wo, egb, eub, edb, dwb,
    qs, kn, nv, att, pa, pb, nsb, sc, snd, rcv, snd2, rcv2, dtok, dps, dpr, fin_s, fin_r,
    load_sem, k_sem, v_sem, own_sem, zs_sem, zr_sem, ps_sem, pr_sem, es_sem, er_sem,
    xs_sem, xr_sem, ms_sem, mr_sem, ts_sem, tr_sem, bs_sem, br_sem, cs_sem, cr_sem,
    fs_sem, fr_sem, line_sem,
):
    ep = lax.axis_index("ep")
    c = lax.axis_index("tp")
    z = ep // 16
    y = (ep // 4) % 4
    x = ep % 4
    other = (ep, 1 - c)
    selfish = c == 0

    def chip(dz, dy, dx):
        return ((z + dz + NZ) % NZ) * 16 + ((y + dy) % 4) * 4 + (x + dx) % 4

    partners = []
    for p, dz in ((0, 0), (1, -1), (2, 1)):
        for dy in (2, 1, 3, 0):
            for dx in (2, 1, 3, 0):
                back = ((3 - p) % 3) * 16 + ((4 - dy) % 4) * 4 + (4 - dx) % 4
                partners.append((chip(4 * c + dz, dy, dx), p * 16 + dy * 4 + dx, back))
    for h in range(2):
        for dy in (2, 1, 3, 0):
            for j in range(2):
                back = 48 + (1 - h) * 8 + ((4 - dy) % 4) * 2 + (c + j) % 2
                partners.append((chip(2 + 4 * h, dy, c + 2 * j), 48 + h * 8 + dy * 2 + j, back))
    plane = []
    for dy in (2, 1, 3, 0):
        for j in range(2):
            plane.append((chip(0, dy, c + 2 * j), dy * 2 + j, ((4 - dy) % 4) * 2 + (c + j) % 2))

    def z_peer(d):
        return (((z + d) % NZ) * 16 + y * 4 + x, c)

    loads = [
        pltpu.make_async_copy(src, dst, load_sem.at[i])
        for i, (src, dst) in enumerate(
            [(w_query, wq), (w_key, wk), (w_value, wv), (w_out, wo),
             (e_gate, egb.at[c]), (e_up, eub.at[c]), (e_down, edb.at[c])]
        )
    ]
    own_parts = [
        pltpu.make_async_copy(src, dwb.at[z, c, i], own_sem.at[i])
        for i, src in enumerate([d_gate, d_up, d_down])
    ]
    kv = []
    for quarter in range(4):
        part = pl.ds(4 * quarter, 4)
        kv.append(
            (
                pltpu.make_async_copy(cache_keys.at[part], kbuf.at[part], k_sem.at[quarter]),
                pltpu.make_async_copy(cache_values.at[part], vbuf.at[part], v_sem.at[quarter]),
            )
        )
    small = [
        pltpu.make_async_copy(src, dst, in_sem.at[i])
        for i, (src, dst) in enumerate(
            [(residual_h, residual), (attend_gain_h, attend_gain), (frequency_h, frequency),
             (lengths_h, lengths), (lambdas_h, lambdas), (routes_h, routes_turned),
             (weights_h, weight_turned), (channel_gain_h, channel_gain), (mixer_h, mixer),
             (head_gain_h, head_gain)]
        )
    ]
    for cp in own_parts + small[:5]:
        cp.start()
    for i in range(3):
        loads[i].start()

    barrier = pltpu.get_barrier_semaphore()
    for d in (4, 3, 5, 2, 6, 1, 7):
        pl.semaphore_signal(barrier, inc=1, device_id=z_peer(d), device_id_type=MESH)
    for k in range(15, 0, -1):
        pl.semaphore_signal(
            barrier, inc=1, device_id=(chip(0, k // 4, k % 4), c), device_id_type=MESH
        )
    pl.semaphore_signal(barrier, inc=1, device_id=other, device_id_type=MESH)

    for keys, values in kv:
        keys.start()
        values.start()
    for cp in small[5:]:
        cp.start()
    loads[3].start()

    for cp in small[:5]:
        cp.wait()
    res = residual[...].astype(F32)
    normed = norm(res, attend_gain[...].astype(F32).reshape(1, WIDTH)).astype(BF)
    for i in range(3):
        loads[i].wait()
    q = jnp.dot(normed, wq[...], preferred_element_type=F32)
    kk = jnp.dot(normed, wk[...], preferred_element_type=F32)
    vv = jnp.dot(normed, wv[...], preferred_element_type=F32).astype(BF)
    lane128 = lax.broadcasted_iota(jnp.int32, (SEQS, 128), 1)
    row16 = lax.broadcasted_iota(jnp.int32, (SEQS, 128), 0)
    first = (lane128 % 64) < 32
    place = jnp.zeros((SEQS, 128), jnp.int32)
    for s in range(SEQS):
        place = jnp.where(row16 == s, lengths[s], place)
    angles = place.astype(F32) * frequency[...]
    cos_t, sin_t = jnp.cos(angles), jnp.sin(angles)
    sin_t = jnp.where(first, -sin_t, sin_t)

    def rotated(u):
        swapped = jnp.where(first, pltpu.roll(u, 96, 1), pltpu.roll(u, 32, 1))
        return (u * cos_t + swapped * sin_t).astype(BF)

    k_rot = rotated(kk)
    new_keys[...] = k_rot
    new_values[...] = vv
    results = [
        pltpu.make_async_copy(new_keys, new_keys_h, out_sem.at[0]),
        pltpu.make_async_copy(new_values, new_values_h, out_sem.at[1]),
    ]
    for cp in results:
        cp.start()
    kn[...] = k_rot.astype(F32)
    nv[...] = vv.astype(F32)
    for g in range(2):
        q_rot = rotated(q[:, 128 * g : 128 * g + 128]).astype(F32) * 0.125
        qs[pl.ds(g, SEQS, stride=4), :] = jnp.where(lane128 < 64, q_rot, 0.0)
        qs[pl.ds(2 + g, SEQS, stride=4), :] = jnp.where(lane128 < 64, 0.0, q_rot)

    pl.semaphore_wait(barrier, 7 + 15 + 1)
    for d in (4, 3, 5, 2, 6, 1, 7):
        pl.semaphore_signal(line_sem, inc=1, device_id=z_peer(d), device_id_type=MESH)

    moved = []

    def z_send(d, hop, part):
        ref = dwb.at[(z + hop + d) % NZ, c, part]
        copy = pltpu.make_async_remote_copy(
            src_ref=ref, dst_ref=ref, send_sem=zs_sem.at[d, part], recv_sem=zr_sem.at[d, part],
            device_id=z_peer(hop), device_id_type=MESH,
        )
        copy.start()
        moved.append(copy)

    def z_wait(d, part):
        ref = dwb.at[(z + d) % NZ, c, part]
        pltpu.make_async_copy(ref, ref, zr_sem.at[d, part]).wait()

    def relay(part):
        z_wait(7, part)
        z_wait(1, part)
        z_send(6, 1, part)
        z_send(2, -1, part)

    def forward(d):
        ref = dwb.at[(z + d) % NZ, c]
        return pltpu.make_async_remote_copy(
            src_ref=ref, dst_ref=ref, send_sem=ps_sem.at[d], recv_sem=pr_sem.at[d],
            device_id=other, device_id_type=MESH,
        )

    for cp in own_parts:
        cp.wait()
    for part in range(3):
        z_send(7, 1, part)
        z_send(1, -1, part)
    z_send(6, 2, 0)
    z_send(2, -2, 0)
    swaps = [
        pltpu.make_async_remote_copy(
            src_ref=src, dst_ref=dst.at[c], send_sem=es_sem.at[i], recv_sem=er_sem.at[i],
            device_id=other, device_id_type=MESH,
        )
        for i, (src, dst) in enumerate([(e_gate, egb), (e_up, eub), (e_down, edb)])
    ]
    forward(0).start()

    sub8 = lax.broadcasted_iota(jnp.int32, (8, 1), 0)
    low8 = sub8 < 4
    lam = jnp.where(sub8 % 2 == 0, lambdas[0], lambdas[1])
    position = lax.broadcasted_iota(jnp.int32, (8, LENGTH), 1)
    turned = (((1,), (1,)), ((), ()))

    def attend(pairs):
        for quarter in sorted({p // 2 for p in pairs}):
            kv[quarter][0].wait()
        scores, own = [], []
        for p in pairs:
            query = qs[8 * p : 8 * p + 8, :]
            first_q = jnp.where(low8, query, 0.0).astype(BF)
            second_q = jnp.where(low8, 0.0, query).astype(BF)
            scores.append(
                lax.dot_general(first_q, kbuf[2 * p], turned, preferred_element_type=F32)
                + lax.dot_general(second_q, kbuf[2 * p + 1], turned, preferred_element_type=F32)
            )
            key = jnp.where(low8, kn[2 * p : 2 * p + 1, :], kn[2 * p + 1 : 2 * p + 2, :])
            own.append(
                jnp.exp(jnp.broadcast_to(jnp.sum(query * key, axis=-1, keepdims=True), (8, 128)))
            )
        weights, own_weights = [], []
        for i, p in enumerate(pairs):
            limit = jnp.where(low8, lengths[2 * p], lengths[2 * p + 1])
            e = jnp.where(position < limit, jnp.exp(scores[i]), 0.0)
            inverse = 1.0 / (jnp.sum(e, axis=-1, keepdims=True) + own[i])
            share = e * inverse[:, 0:1]
            share_own = own[i] * inverse
            weights.append((share - lam * pltpu.roll(share, 6, 0)).astype(BF))
            own_weights.append(
                (share_own - lam * pltpu.roll(share_own, 6, 0)).astype(BF).astype(F32)
            )
        for quarter in sorted({p // 2 for p in pairs}):
            kv[quarter][1].wait()
        for i, p in enumerate(pairs):
            first_a = jnp.dot(weights[i], vbuf[2 * p], preferred_element_type=F32)
            second_a = jnp.dot(weights[i], vbuf[2 * p + 1], preferred_element_type=F32)
            value = jnp.where(low8, nv[2 * p : 2 * p + 1, :], nv[2 * p + 1 : 2 * p + 2, :])
            att[8 * p : 8 * p + 8, :] = (
                jnp.where(low8, first_a, second_a) + own_weights[i] * value
            )

    attend((0, 1))

    attend((2, 3))
    attend((4, 5, 6, 7))

    for i in range(4, 7):
        loads[i].start()

    for cp in small[5:]:
        cp.wait()
    gain_h = head_gain[...].astype(F32).reshape(1, 128)
    rows = jnp.concatenate(
        [(norm(att[pl.ds(g, SEQS, stride=4), :], gain_h) * 0.8).astype(BF) for g in range(2)], axis=1
    )
    loads[3].wait()
    pa[...] = jnp.dot(rows, wo[...], preferred_element_type=F32).astype(BF)
    swap_a = pltpu.make_async_remote_copy(
        src_ref=pa, dst_ref=pb, send_sem=xs_sem, recv_sem=xr_sem,
        device_id=other, device_id_type=MESH,
    )
    swap_a.start()
    for cp in swaps:
        cp.start()

    row128 = lax.broadcasted_iota(jnp.int32, (128, SEQS), 0)
    block = row128 // 2
    in_half = block >= 48
    third = block // 16
    dz_t = jnp.where(in_half, 2 + 4 * ((block // 8) % 2), 4 * c + jnp.where(third == 2, 1, -third))
    dy_t = jnp.where(in_half, (block // 2) % 4, (block // 4) % 4)
    dx_t = jnp.where(in_half, c + 2 * (block % 2), block % 4)
    expert_t = ((z + dz_t + NZ) % NZ) * 16 + ((y + dy_t) % 4) * 4 + (x + dx_t) % 4
    hit_t = jnp.zeros((128, SEQS), F32)
    weight_t = jnp.zeros((128, SEQS), F32)
    for k in range(6):
        same = routes_turned[k : k + 1, :] == expert_t
        hit_t = hit_t + jnp.where(same, 1.0, 0.0)
        weight_t = weight_t + jnp.where(same, weight_turned[k : k + 1, :], 0.0)
    up_tri = jnp.where(
        lax.broadcasted_iota(jnp.int32, (SEQS, SEQS), 0)
        < lax.broadcasted_iota(jnp.int32, (SEQS, SEQS), 1),
        1.0, 0.0,
    )
    rank_t = jnp.dot(hit_t.astype(BF), up_tri.astype(BF), preferred_element_type=F32)
    pick_t = jnp.where(rank_t == (row128 % 2).astype(F32), hit_t, 0.0).astype(BF)

    combine_t = jnp.where(rank_t == (row128 % 2).astype(F32), weight_t, 0.0)
    c_hi = combine_t.astype(BF)
    rest = combine_t - c_hi.astype(F32)
    c_mid = rest.astype(BF)
    c_lo = (rest - c_mid.astype(F32)).astype(BF)
    eye = jnp.where(
        lax.broadcasted_iota(jnp.int32, (SEQS, SEQS), 0)
        == lax.broadcasted_iota(jnp.int32, (SEQS, SEQS), 1),
        1.0, 0.0,
    ).astype(BF)
    combine3 = jnp.concatenate(
        [
            lax.dot_general(eye, part, (((1,), (1,)), ((), ())), preferred_element_type=F32)
            for part in (c_hi, c_mid, c_lo)
        ],
        axis=0,
    ).astype(BF)

    relay(1)
    swap_a.wait()
    relay(2)
    middle = (res + (pa[...].astype(F32) + pb[...].astype(F32))).astype(BF).astype(F32)
    ns = norm(middle, channel_gain[...].astype(F32).reshape(1, WIDTH)).astype(BF)
    nsb[...] = ns
    switch = jax.nn.sigmoid(
        jnp.sum(ns.astype(F32) * mixer[...].astype(F32).reshape(1, WIDTH), axis=-1, keepdims=True)
    )

    def spread(values):
        for j in range(8):
            sc[pl.ds(j, 128, stride=8), :] = values[:, 128 * j : 128 * j + 128]

    def send_each(peers, pick_src, dst, send_sem, recv_sem):
        for target, here, there in peers:
            remote = pltpu.make_async_remote_copy(
                src_ref=pick_src(here), dst_ref=dst.at[there], send_sem=send_sem,
                recv_sem=recv_sem, device_id=(target, c), device_id_type=MESH,
            )
            if here:
                remote.start()
                continue

            @pl.when(selfish)
            def _():
                pltpu.make_async_copy(pick_src(0), dst.at[0], recv_sem).start()

            @pl.when(jnp.logical_not(selfish))
            def _(remote=remote):
                remote.start()

    def sent_all(buf, send_sem, count):
        @pl.when(selfish)
        def _():
            part = buf.at[pl.ds(0, count - 1)]
            pltpu.make_async_copy(part, part, send_sem).wait()

        @pl.when(jnp.logical_not(selfish))
        def _():
            pltpu.make_async_copy(buf, buf, send_sem).wait()

    picked = jnp.dot(pick_t, ns, preferred_element_type=F32)
    for j in range(8):
        sc[pl.ds(j, 128, stride=8), :] = picked[:, 128 * j : 128 * j + 128]
    snd[...] = sc[...].reshape(64, 16, 128).astype(BF)
    pl.semaphore_wait(line_sem, 7)
    send_each(partners, lambda n: snd.at[n], rcv, ms_sem, mr_sem)
    send_each(plane, lambda n: nsb, dtok, ts_sem, tr_sem)

    z_wait(7, 0)
    z_wait(1, 0)
    forward(7).start()
    forward(1).start()
    for part in range(3):
        z_wait(6, part)
        z_send(5, 1, part)
        z_wait(2, part)
        z_send(3, -1, part)
    for part in range(3):
        z_send(4, 2 - 4 * c, part)
    forward(6).start()
    forward(2).start()

    for i in range(4, 7):
        loads[i].wait()
    for cp in swaps:
        cp.wait()

    pltpu.make_async_copy(rcv, rcv, mr_sem).wait()
    sc[...] = rcv[...].reshape(1024, 128).astype(F32)
    rows = jnp.concatenate(
        [sc[pl.ds(j, 128, stride=8), :].astype(BF) for j in range(8)], axis=1
    )
    total = None
    for h in range(2):
        gate = jnp.dot(rows, egb[h], preferred_element_type=F32)
        upper = jnp.dot(rows, eub[h], preferred_element_type=F32)
        hidden = (silu(gate) * upper).astype(BF)
        half = jnp.dot(hidden, edb[h], preferred_element_type=F32).astype(BF).astype(F32)
        total = half if total is None else total + half
    for j in range(8):
        sc[pl.ds(j, 128, stride=8), :] = total[:, 128 * j : 128 * j + 128]
    snd2[...] = sc[...].reshape(64, 16, 128).astype(BF)
    send_each(partners, lambda n: snd2.at[n], rcv2, bs_sem, br_sem)

    for d in (3, 5, 4):
        for part in range(3):
            z_wait(d, part)
        forward(d).start()
    pltpu.make_async_copy(dtok, dtok, tr_sem).wait()
    for d in range(8):
        mirror = dwb.at[(z + d) % NZ, 1 - c]
        pltpu.make_async_copy(mirror, mirror, pr_sem.at[d]).wait()
    xd = dtok[...].reshape(128, WIDTH)
    gate_w = dwb[:, :, 0].reshape(256, WIDTH)
    up_w = dwb[:, :, 1].reshape(256, WIDTH)
    down_w = dwb[:, :, 2].reshape(256, WIDTH)
    gate = lax.dot_general(xd, gate_w, turned, preferred_element_type=F32)
    upper = lax.dot_general(xd, up_w, turned, preferred_element_type=F32)
    hidden = (silu(gate) * upper).astype(BF)
    dps[...] = jnp.dot(hidden, down_w, preferred_element_type=F32).astype(BF).reshape(8, 16, WIDTH)
    send_each(plane, lambda n: dps.at[n], dpr, cs_sem, cr_sem)

    pltpu.make_async_copy(rcv2, rcv2, br_sem).wait()
    sc[...] = rcv2[...].reshape(1024, 128).astype(F32)
    returned = jnp.concatenate(
        [sc[pl.ds(j, 128, stride=8), :].astype(BF) for j in range(8)], axis=1
    )
    three = jnp.dot(combine3, returned, preferred_element_type=F32)
    routed = three[0:16] + (three[16:32] + three[32:48])
    pltpu.make_async_copy(dpr, dpr, cr_sem).wait()
    dense = dpr[0].astype(F32)
    for i in range(1, 8):
        dense = dense + dpr[i].astype(F32)
    fin_s[...] = routed + switch * dense
    swap_f = pltpu.make_async_remote_copy(
        src_ref=fin_s, dst_ref=fin_r, send_sem=fs_sem, recv_sem=fr_sem,
        device_id=other, device_id_type=MESH,
    )
    swap_f.start()
    sent_all(snd, ms_sem, 64)
    sent_all(snd2, bs_sem, 64)
    sent_all(dtok, ts_sem, 8)
    sent_all(dps, cs_sem, 8)
    for cp in moved:
        cp.wait_send()
    for d in range(8):
        forward(d).wait_send()
    swap_f.wait()
    out[...] = (middle + (fin_s[...] + fin_r[...])).astype(BF)
    last = pltpu.make_async_copy(out, out_h, out_sem.at[2])
    last.start()
    for cp in results + [last]:
        cp.wait()


def hand_over(a, b, c, a_out, b_out, c_out):
    a_out[...] = a[...]
    b_out[...] = b[...]
    c_out[...] = c[...]


def per_device(
    residual_in, lengths, cache_keys, cache_values, attend_gain, query_proj, key_proj,
    value_proj, lambdas, head_gain, out_proj, channel_gain, routes, route_weight,
    expert_gate, expert_up, expert_down, dense_gate, dense_up, dense_down, dense_mixer,
):
    inverse = np.float32(10000.0) ** (-np.arange(32, dtype=np.float32) / np.float32(32))
    frequency = jnp.asarray(np.tile(inverse, 4)[None, :])
    vm = pl.BlockSpec(memory_space=pltpu.VMEM)
    hb = pl.BlockSpec(memory_space=pl.ANY)
    DMA = pltpu.SemaphoreType.DMA
    V = pltpu.VMEM
    out, keys, values = pl.pallas_call(
        body,
        name="layer",
        out_shape=(
            jax.ShapeDtypeStruct((SEQS, WIDTH), BF),
            jax.ShapeDtypeStruct((SEQS, 128), BF),
            jax.ShapeDtypeStruct((SEQS, 128), BF),
        ),
        in_specs=[hb] * 22,
        out_specs=(hb, hb, hb),
        scratch_shapes=[
            V((SEQS, WIDTH), BF), V((WIDTH,), BF), V((WIDTH,), BF), V((WIDTH,), BF),
            V((128,), BF), V((1, 128), F32), pltpu.SMEM((SEQS,), jnp.int32),
            pltpu.SMEM((2,), F32), V((6, SEQS), jnp.int32), V((6, SEQS), F32),
            V((SEQS, WIDTH), BF), V((SEQS, 128), BF), V((SEQS, 128), BF), DMA((10,)), DMA((3,)),
            V((SEQS, LENGTH, 128), BF), V((SEQS, LENGTH, 128), BF),
            V((1024, 256), BF), V((1024, 128), BF), V((1024, 128), BF), V((256, 1024), BF),
            V((2, 1024, 256), BF), V((2, 1024, 256), BF), V((2, 256, 1024), BF),
            V((8, 2, 3, 16, 1024), BF),
            V((64, 128), F32), V((SEQS, 128), F32), V((SEQS, 128), F32),
            V((64, 128), F32),
            V((SEQS, WIDTH), BF), V((SEQS, WIDTH), BF), V((SEQS, WIDTH), BF),
            V((1024, 128), F32),
            V((64, 16, 128), BF), V((64, 16, 128), BF), V((64, 16, 128), BF), V((64, 16, 128), BF),
            V((8, 16, WIDTH), BF), V((8, 16, WIDTH), BF), V((8, 16, WIDTH), BF),
            V((SEQS, WIDTH), F32), V((SEQS, WIDTH), F32),
            DMA((7,)), DMA((4,)), DMA((4,)), DMA((3,)),
            DMA((8, 3)), DMA((8, 3)), DMA((8,)), DMA((8,)), DMA((3,)), DMA((3,)),
            DMA, DMA, DMA, DMA, DMA, DMA, DMA, DMA, DMA, DMA,
            DMA, DMA, pltpu.SemaphoreType.REGULAR,
        ],
        compiler_params=pltpu.CompilerParams(
            collective_id=0, has_side_effects=True, vmem_limit_bytes=60 * 1024 * 1024,
        ),
    )(
        residual_in, attend_gain, channel_gain, dense_mixer, head_gain, frequency,
        lengths, lambdas, routes.T, route_weight.T,
        cache_keys.reshape(SEQS, LENGTH, 128), cache_values.reshape(SEQS, LENGTH, 128),
        query_proj, key_proj, value_proj, out_proj,
        expert_gate[0], expert_up[0], expert_down[0], dense_gate.T, dense_up.T, dense_down,
    )
    out, keys, values = pl.pallas_call(
        hand_over,
        name="hand_over",
        out_shape=(
            jax.ShapeDtypeStruct((SEQS, WIDTH), BF),
            jax.ShapeDtypeStruct((SEQS, 128), BF),
            jax.ShapeDtypeStruct((SEQS, 128), BF),
        ),
        in_specs=[vm] * 3,
        out_specs=(vm, vm, vm),
    )(out, keys, values)
    return out, keys.reshape(SEQS, 1, 128), values.reshape(SEQS, 1, 128)


def solution(mesh):
    placed = (
        P("ep", None), P("ep"), P("ep", "tp", None, None), P("ep", "tp", None, None), P(),
        P(None, "tp"), P(None, "tp"), P(None, "tp"), P("tp"), P(), P("tp", None), P(),
        P("ep", None), P("ep", None), P("ep", None, "tp"), P("ep", None, "tp"),
        P("ep", "tp", None), P(None, ("ep", "tp")), P(None, ("ep", "tp")),
        P(("ep", "tp"), None), P(),
    )
    return jax.shard_map(
        per_device, mesh=mesh, in_specs=placed,
        out_specs=(P("ep", None), P("ep", "tp", None), P("ep", "tp", None)),
        check_vma=False,
    )
```
